32 devices in a mesh: sp: 4 (over x, core), dp: 8 (over z, y).
Axes of the slice: x: 2, y: 2, z: 4, core: 2. Of those that a mesh axis runs over, the one named last changes fastest.
Arguments:
- query: bfloat16 [8, 512, 1024], P('dp', None, 'sp'), may hold values from -120 to 120
- keys: bfloat16 [8, 512, 1024], P('dp', None, 'sp'), may hold values from -6 to 6
- values: bfloat16 [8, 512, 1024], P('dp', None, 'sp'), may hold values from -6 to 6
- output: bfloat16 [8, 512, 1024], P('dp'), may hold values from -1 to 1
- cum: float32 [8, 16, 512], P('dp', 'sp'), as said below
- d_out: bfloat16 [8, 512, 2048], P('dp', 'sp'), may hold values from -6 to 6
- w_out: bfloat16 [1024, 2048], P('dp'), may hold values from -0.125 to 0.125
Outputs:
- d_query: bfloat16 [8, 512, 1024], P('dp', 'sp')
- d_key: bfloat16 [8, 512, 1024], P('dp', 'sp')
- d_value: bfloat16 [8, 512, 1024], P('dp', 'sp')
- d_cum: float32 [8, 16, 512], P('dp', 'sp')
- d_w_out: float32 [1024, 2048], P('dp', 'sp')
The draws below stay inside these ranges and needn't reach their ends.
Inputs may be any that keep to these rules, and one draw needn't show every extreme that they name: cum never rises along positions.
All inputs are finite; a program needn't handle non-finite values.
Results may differ from the reference program's by a relative error of at most 0.008.
Values may be sent and summed in bfloat16 or wider, within the bound.
A program may use at most 64 MiB of HBM per device.

```python
import jax
import jax.numpy as jnp
from jax import lax

D = 2048
HEAD_TOTAL = 16
HEAD = 64
TOK_DEV = 128
ATTN = 1024
SEQUENCE_LENGTH = 512
SEQUENCE_COUNT = 8


def shared_keys(key):
    return jnp.clip(jax.random.normal(jax.random.fold_in(key, 11), (SEQUENCE_COUNT, SEQUENCE_LENGTH, ATTN), jnp.float32), -6.0, 6.0)


def draw_keys(key, part):
    return shared_keys(key).astype(jnp.bfloat16)


def draw_query(key, part):
    base_query = jnp.clip(jax.random.normal(jax.random.fold_in(key, 12), (SEQUENCE_COUNT, SEQUENCE_LENGTH, ATTN), jnp.float32), -6.0, 6.0)
    return base_query.astype(jnp.bfloat16)


def draw_cum(key, part):
    shape = (SEQUENCE_COUNT, HEAD_TOTAL, SEQUENCE_LENGTH)
    slow_share = 0.5
    slow_heads = jax.random.uniform(jax.random.fold_in(key, 21), (SEQUENCE_COUNT, HEAD_TOTAL, 1)) < slow_share
    fast_rate = jnp.exp(jax.random.uniform(jax.random.fold_in(key, 22), (SEQUENCE_COUNT, HEAD_TOTAL, 1), jnp.float32, jnp.log(1.0 / 60.0), jnp.log(1.0 / 25.0)))
    slow_rate = 0.7 / SEQUENCE_LENGTH * jnp.exp(jax.random.uniform(jax.random.fold_in(key, 23), (SEQUENCE_COUNT, HEAD_TOTAL, 1), jnp.float32, -0.7, 0.7))
    blocks = SEQUENCE_LENGTH // TOK_DEV
    block_factor = jnp.exp(jax.random.uniform(jax.random.fold_in(key, 24), (SEQUENCE_COUNT, HEAD_TOTAL, blocks), jnp.float32, -0.7, 0.7))
    block_factor = jnp.repeat(block_factor, TOK_DEV, axis=2)
    roughness = jax.random.uniform(jax.random.fold_in(key, 25), shape, jnp.float32, 0.3, 1.7)
    decay_rates = jnp.where(slow_heads, slow_rate, fast_rate) * block_factor * roughness
    spike_positions = jax.random.randint(jax.random.fold_in(key, 26), (SEQUENCE_COUNT, HEAD_TOTAL, 3), 0, SEQUENCE_LENGTH)
    spike_length = jnp.log(1.0 - jax.random.uniform(jax.random.fold_in(key, 27), (SEQUENCE_COUNT, HEAD_TOTAL, 3), jnp.float32, 0.2, 0.5))
    locations = jnp.arange(SEQUENCE_LENGTH)
    spikes = jnp.sum(jnp.where(locations[None, None, None, :] == spike_positions[:, :, :, None], spike_length[:, :, :, None], 0.0), axis=2)
    return jnp.cumsum(spikes - decay_rates, axis=2)


def raised(result, key, source, target, shards_of, factor):
    owner, partner = [(jnp.arange(result.shape[dim]) // (result.shape[dim] // shards_of)).reshape([-1 if axis == dim else 1 for axis in range(result.ndim)]) for dim in (source, target)]
    chosen = jax.random.permutation(key, shards_of)[partner]
    strong = (owner == chosen) | (owner == (partner + shards_of // 2) % shards_of)
    return jnp.where(strong, factor * result, result)


def level_of(rng, dims, pieces, low, high):
    factor_of, own = 1.0, jax.random.fold_in(rng, 6)
    for axis_at, parts in pieces:
        steps = jnp.exp(jax.random.uniform(jax.random.fold_in(own, axis_at), (parts,), jnp.float32, low / len(pieces), high / len(pieces)))
        factor_of = factor_of * jnp.repeat(steps, dims[axis_at] // parts).reshape([-1 if axis == axis_at else 1 for axis in range(len(dims))])
    return factor_of


def gaussian(stream_key, shape, width, bound, cuts=(), kind=jnp.bfloat16):
    array = jax.random.normal(stream_key, shape, jnp.float32) * width
    if len(cuts) > 0:
        array = level_of(stream_key, shape, cuts, -0.22, 0.18) * array
    return jnp.clip(array, min=-bound, max=bound).astype(kind)


def heavy_noise(key, extent, spread, limit, pieces, heavy, kind=jnp.bfloat16):
    array = spread * jax.random.normal(key, extent, jnp.float32)
    if pieces:
        array = array * level_of(key, extent, pieces, -0.22, 0.18)
    return jnp.clip(raised(array, jax.random.fold_in(key, 3), *heavy), -limit, limit).astype(kind)


def setup_inputs(seed: int = 0) -> dict:
    seeds = jax.random.split(jax.random.key(seed), 8)
    query = draw_query(jax.random.fold_in(seeds[7], 71), 0)
    keys = draw_keys(jax.random.fold_in(seeds[7], 71), 0)
    values = gaussian(seeds[2], (SEQUENCE_COUNT, SEQUENCE_LENGTH, ATTN), 1.0, 6.0, ((0, 8), (2, 4)))
    output = heavy_noise(seeds[3], (SEQUENCE_COUNT, SEQUENCE_LENGTH, ATTN), 0.125, 1.0, ((0, 8),), (0, 2, 8, 2.0))
    cum = draw_cum(jax.random.fold_in(seeds[7], 71), 0)
    d_out = gaussian(seeds[5], (SEQUENCE_COUNT, SEQUENCE_LENGTH, D), 1.0, 6.0, ((0, 8), (1, 4)))
    w_out = gaussian(seeds[6], (ATTN, D), D ** -0.5, 0.125, ((0, 8),))
    return {"query": query, "keys": keys, "values": values, "output": output, "cum": cum, "d_out": d_out, "w_out": w_out}


def product(left, right, form):
    return jnp.einsum(form, left.astype(jnp.float32), right.astype(jnp.float32))


def head_grads(query, keys, values, output, cotangent, cum):
    head_count, length, head_width = query.shape
    span_rows = min(512, length)
    score_scale = head_width ** -0.5
    row_dots = jnp.sum(cotangent.astype(jnp.float32) * output.astype(jnp.float32), axis=2)
    positions = jnp.arange(length)

    def advance(totals, block_index):
        key_grad, value_grad, cum_grad = totals
        offset = (block_index * span_rows).astype(jnp.int32)
        query_blk = lax.dynamic_slice_in_dim(query, offset, span_rows, 1)
        cot_blk = lax.dynamic_slice_in_dim(cotangent, offset, span_rows, 1)
        cum_blk = lax.dynamic_slice_in_dim(cum, offset, span_rows, 1)
        dots_blk = lax.dynamic_slice_in_dim(row_dots, offset, span_rows, 1)
        scores = product(query_blk, keys, "hqe,hke->hqk") * score_scale
        scores = scores + cum_blk[:, :, None] - cum[:, None, :]
        query_pos = offset + jnp.arange(span_rows)
        causal = positions[None, :] <= query_pos[:, None]
        scores = jnp.where(causal[None], scores, -1e30)
        row_max = jnp.max(scores, axis=2, keepdims=True)
        weights = jnp.exp(scores - row_max)
        weights = weights / jnp.sum(weights, axis=2, keepdims=True)
        weights_b = weights.astype(jnp.bfloat16)
        d_prob = product(cot_blk, values, "hqe,hke->hqk")
        d_score = weights * (d_prob - dots_blk[:, :, None])
        score_b = d_score.astype(jnp.bfloat16)
        query_grad = (product(score_b, keys, "hqk,hke->hqe") * score_scale).astype(jnp.bfloat16)
        key_grad = key_grad + product(score_b, query_blk, "hqk,hqe->hke") * score_scale
        value_grad = value_grad + product(weights_b, cot_blk, "hqk,hqe->hke")
        cum_grad = cum_grad - jnp.sum(d_score, axis=1)
        own_part = lax.dynamic_slice_in_dim(cum_grad, offset, span_rows, 1) + jnp.sum(d_score, axis=2)
        cum_grad = lax.dynamic_update_slice_in_dim(cum_grad, own_part, offset, 1)
        return (key_grad, value_grad, cum_grad), query_grad

    start_state = (jnp.zeros(query.shape, jnp.float32), jnp.zeros(query.shape, jnp.float32),
                   jnp.zeros(cum.shape, jnp.float32))
    totals, query_blocks = lax.scan(advance, start_state, jnp.arange(length // span_rows))
    query_grad = jnp.transpose(query_blocks, (1, 0, 2, 3)).reshape(query.shape)
    return query_grad, totals[0].astype(jnp.bfloat16), totals[1].astype(jnp.bfloat16), totals[2]


def reference(query, keys, values, output, cum, d_out, w_out):
    def one_sequence(sequence):
        q_seq, k_seq, v_seq, o_seq, c_seq, g_seq = sequence
        d_attn = jnp.dot(g_seq, w_out.T, preferred_element_type=jnp.float32).astype(jnp.bfloat16)

        def heads_first(matrix):
            return jnp.transpose(matrix.reshape(SEQUENCE_LENGTH, HEAD_TOTAL, HEAD), (1, 0, 2))

        def tokens_first(matrix):
            return jnp.transpose(matrix, (1, 0, 2)).reshape(SEQUENCE_LENGTH, ATTN)

        grads = head_grads(heads_first(q_seq), heads_first(k_seq), heads_first(v_seq),
                           heads_first(o_seq), heads_first(d_attn), c_seq)
        return tokens_first(grads[0]), tokens_first(grads[1]), tokens_first(grads[2]), grads[3]

    d_query, d_key, d_value, d_cum = lax.map(one_sequence, (query, keys, values, output, cum, d_out))

    def accumulate(running, couple):
        return running + jnp.dot(couple[0].T, couple[1], preferred_element_type=jnp.float32), None

    d_w_out = lax.scan(accumulate, jnp.zeros((ATTN, D), jnp.float32), (output, d_out))[0]
    return d_query, d_key, d_value, d_cum, d_w_out
```

```python
import contextlib
import functools

import jax
import jax.numpy as jnp
from jax import lax
from jax.experimental import pallas as pl
from jax.experimental.pallas import tpu as pltpu
from jax.sharding import PartitionSpec as P


def head_grads(query, keys, values, output, cotangent, cum):
    head_count, length, head_width = query.shape
    span_rows = min(512, length)
    score_scale = head_width ** (-0.5)
    row_dots = jnp.sum(cotangent.astype(jnp.float32) * output.astype(jnp.float32), axis=2)
    positions = jnp.arange(length)

    def product(left, right, form):
        return jnp.einsum(form, left, right, preferred_element_type=jnp.float32)

    def advance(totals, block_index):
        key_grad, value_grad, cum_grad = totals
        offset = block_index * span_rows
        query_blk = lax.dynamic_slice_in_dim(query, offset, span_rows, 1)
        cot_blk = lax.dynamic_slice_in_dim(cotangent, offset, span_rows, 1)
        cum_blk = lax.dynamic_slice_in_dim(cum, offset, span_rows, 1)
        dots_blk = lax.dynamic_slice_in_dim(row_dots, offset, span_rows, 1)
        scores = product(query_blk, keys, "hqe,hke->hqk") * score_scale
        scores = scores + cum_blk[:, :, None] - cum[:, None, :]
        query_pos = offset + jnp.arange(span_rows)
        causal = positions[None, :] <= query_pos[:, None]
        scores = jnp.where(causal[None], scores, -1e30)
        row_max = jnp.max(scores, axis=2, keepdims=True)
        weights = jnp.exp(scores - row_max)
        weights = weights / jnp.sum(weights, axis=2, keepdims=True)
        weights_b = weights.astype(jnp.bfloat16)
        d_prob = product(cot_blk, values, "hqe,hke->hqk")
        d_score = weights * (d_prob - dots_blk[:, :, None])
        score_b = d_score.astype(jnp.bfloat16)
        query_grad = (product(score_b, keys, "hqk,hke->hqe") * score_scale).astype(jnp.bfloat16)
        key_grad = key_grad + product(score_b, query_blk, "hqk,hqe->hke") * score_scale
        value_grad = value_grad + product(weights_b, cot_blk, "hqk,hqe->hke")
        cum_grad = cum_grad - jnp.sum(d_score, axis=1)
        own_part = lax.dynamic_slice_in_dim(cum_grad, offset, span_rows, 1) + jnp.sum(
            d_score, axis=2
        )
        cum_grad = lax.dynamic_update_slice_in_dim(cum_grad, own_part, offset, 1)
        return ((key_grad, value_grad, cum_grad), query_grad)

    start_state = (
        jnp.zeros(query.shape, jnp.float32),
        jnp.zeros(query.shape, jnp.float32),
        jnp.zeros(cum.shape, jnp.float32),
    )
    totals, query_blocks = lax.scan(advance, start_state, jnp.arange(length // span_rows))
    query_grad = jnp.transpose(query_blocks, (1, 0, 2, 3)).reshape(query.shape)
    return (query_grad, totals[0].astype(jnp.bfloat16), totals[1].astype(jnp.bfloat16), totals[2])


def shards(query, keys, values, output, cum, d_out, w_out):
    local_rows = d_out[0]
    whole_output = output[0]
    d_attn = lax.dot_general(
        local_rows,
        lax.all_gather(w_out, "dp", axis=0, tiled=True),
        (((1,), (1,)), ((), ())),
        preferred_element_type=jnp.float32,
    ).astype(jnp.bfloat16)
    head_cot, column_part = (
        lax.all_to_all(d_attn[None], "sp", split_axis=2, concat_axis=1, tiled=True),
        lax.all_to_all(d_out, "sp", split_axis=2, concat_axis=1, tiled=True),
    )
    grad_weight = lax.psum_scatter(
        lax.dot_general(
            whole_output,
            column_part[0],
            (((0,), (0,)), ((), ())),
            preferred_element_type=jnp.float32,
        ),
        "dp",
        scatter_dimension=0,
        tiled=True,
    )
    head_cols = query.shape[2]
    head_count = cum.shape[1]
    head_width = head_cols // head_count
    seq_length = query.shape[1]
    own_output = lax.dynamic_slice_in_dim(
        whole_output, lax.axis_index("sp") * head_cols, head_cols, 1
    )

    def heads_first(matrix):
        return jnp.transpose(matrix.reshape(seq_length, head_count, head_width), (1, 0, 2))

    def tokens_first(matrix):
        return jnp.transpose(matrix, (1, 0, 2)).reshape(1, seq_length, head_cols)

    grads = head_grads(
        heads_first(query[0]),
        heads_first(keys[0]),
        heads_first(values[0]),
        heads_first(own_output),
        heads_first(head_cot[0]),
        cum[0],
    )
    query_grad, key_grad, value_grad = (
        lax.all_to_all(tokens_first(grads[0]), "sp", split_axis=1, concat_axis=2, tiled=True),
        lax.all_to_all(tokens_first(grads[1]), "sp", split_axis=1, concat_axis=2, tiled=True),
        lax.all_to_all(tokens_first(grads[2]), "sp", split_axis=1, concat_axis=2, tiled=True),
    )
    return (query_grad, key_grad, value_grad, grads[3][None], grad_weight)


def plain_solution(mesh):
    placed = (
        P("dp", None, "sp"),
        P("dp", None, "sp"),
        P("dp", None, "sp"),
        P("dp", None, None),
        P("dp", "sp", None),
        P("dp", "sp", None),
        P("dp", None),
    )
    return jax.shard_map(
        shards,
        mesh=mesh,
        in_specs=placed,
        out_specs=(
            P("dp", "sp", None),
            P("dp", "sp", None),
            P("dp", "sp", None),
            P("dp", "sp", None),
            P("dp", "sp"),
        ),
        check_vma=False,
    )


MESH = pl.DeviceIdType.MESH
ns = contextlib.nullcontext
PAIR = 2
LANES = 128


def nt(left, right):
    return lax.dot_general(
        left, right, (((1,), (1,)), ((), ())), preferred_element_type=jnp.float32
    )


def nn(left, right):
    return lax.dot_general(
        left, right, (((1,), (0,)), ((), ())), preferred_element_type=jnp.float32
    )


def kernel(
    n_sp, n_dp, n_heads, w_chunks,
    q_hbm, k_hbm, v_hbm, o_hbm, cum_hbm, do_hbm, w_hbm,
    dq_out, dk_out, dv_out, dcum_out, dw_out,
    q_ref, k_ref, v_ref, o_ref, cum_ref, dof, wbuf, prob, prob_b, k_t, o_t,
    dw_part, y_send, y_recv, z_send, z_recv, dw_acc, stage, dcum_ref,
    in_sem, out_sem,
    x_ssem, x_rsem, c_ssem, c_rsem, f_ssem, f_rsem,
    wz_ssem, wz_rsem, wy_ssem, wy_rsem,
    ry_ssem, ry_rsem, rz_ssem, rz_rsem,
    g_ssem, g_rsem, g_lsem,
):
    sp, dp = lax.axis_index("sp"), lax.axis_index("dp")
    n_z = n_dp // PAIR
    x, core = sp // PAIR, sp % PAIR
    z, y = dp // PAIR, dp % PAIR
    length, head_cols = q_ref.shape
    head_width = head_cols // n_heads
    tokens, width = do_hbm.shape[1:]
    w_rows = w_hbm.shape[0]
    col_part = width // n_sp
    scale = head_width ** (-0.5)
    per_pair = LANES // head_width
    n_pairs = head_cols // LANES
    block = min(2 * LANES, length)
    n_blocks = length // block
    core_peer = x * PAIR + (1 - core)
    y_peer = z * PAIR + (1 - y)

    def token_rows(owner):
        return pl.ds(pl.multiple_of(owner * tokens, tokens), tokens)

    def col_at(part):
        return pl.ds(pl.multiple_of(part * col_part, LANES), col_part)

    def remote(src, dst, ssem, rsem, **where):
        return pltpu.make_async_remote_copy(
            src_ref=src, dst_ref=dst, send_sem=ssem, recv_sem=rsem,
            device_id=where, device_id_type=MESH,
        )

    own_w = pl.ds(pl.multiple_of(y * w_rows, w_rows), w_rows)
    loads = [
        pltpu.make_async_copy(do_hbm.at[0], dof.at[token_rows(sp)], in_sem.at[0]),
        pltpu.make_async_copy(q_hbm.at[0], q_ref, in_sem.at[2]),
        pltpu.make_async_copy(k_hbm.at[0], k_ref, in_sem.at[3]),
        pltpu.make_async_copy(cum_hbm.at[0], cum_ref, in_sem.at[4]),
        pltpu.make_async_copy(v_hbm.at[0], v_ref, in_sem.at[5]),
        pltpu.make_async_copy(o_hbm.at[0], o_ref, in_sem.at[6]),
    ]
    w_load = pltpu.make_async_copy(w_hbm, wbuf.at[own_w], in_sem.at[1])
    loads[0].start()

    @pl.when(z == sp)
    def _():
        w_load.start()

    for load in loads[1:]:
        load.start()

    barrier = pltpu.get_barrier_semaphore()
    for off in range(1, n_sp):
        pl.semaphore_signal(
            barrier, inc=1, device_id={"sp": (sp + off) % n_sp, "dp": dp}, device_id_type=MESH
        )
    for off in range(1, n_z):
        pl.semaphore_signal(
            barrier, inc=1,
            device_id={"sp": sp, "dp": ((z + off) % n_z) * PAIR + y}, device_id_type=MESH,
        )
    pl.semaphore_signal(barrier, inc=1, device_id={"sp": sp, "dp": y_peer}, device_id_type=MESH)
    pl.semaphore_wait(barrier, n_sp + n_z - 1)

    def chip_rows(owner_x):
        return pl.ds(pl.multiple_of(owner_x * PAIR * tokens, PAIR * tokens), PAIR * tokens)

    def x_out(i):
        part = dof.at[token_rows(sp), col_at(((1 - x) * PAIR + i) % n_sp)]
        slot, target_core = (0, i) if i < PAIR else (i - 1, core)
        return remote(part, part, x_ssem, x_rsem.at[slot], sp=(1 - x) * PAIR + target_core, dp=dp)

    def arrived(i, owner_core):
        if i == 0:
            return dof.at[chip_rows(1 - x), col_at(x * PAIR + owner_core)]
        owner = (1 - x) * PAIR + owner_core
        return dof.at[token_rows(owner), col_at((x * PAIR + i + 1) % n_sp)]

    def x_in(i):
        part = arrived(i, core)
        return remote(part, part, x_ssem, x_rsem.at[i], sp=core_peer, dp=dp)

    def core_copy(owner):
        part = dof.at[token_rows(owner)]
        return remote(part, part, c_ssem, c_rsem, sp=core_peer, dp=dp)

    def forward_copy(i, owner_core):
        part = arrived(i, owner_core)
        return remote(part, part, f_ssem, f_rsem.at[min(i, 1)], sp=core_peer, dp=dp)

    def x_start():
        loads[0].wait()
        for i in range(n_sp):
            x_out(i).start()

    def forward_step(i):
        x_in(i).wait_recv()
        forward_copy(i, core).start()

    chunk_rows = w_rows // w_chunks

    def w_part(owner_y, c):
        start = pl.multiple_of(owner_y * w_rows + c * chunk_rows, chunk_rows)
        return wbuf.at[pl.ds(start, chunk_rows)]

    def wz_copy(way, c, target_z):
        return remote(w_part(y, c), w_part(y, c), wz_ssem.at[way], wz_rsem.at[c],
                      sp=sp, dp=target_z * PAIR + y)

    def wy_copy(owner_y, c):
        return remote(w_part(owner_y, c), w_part(owner_y, c), wy_ssem, wy_rsem,
                      sp=sp, dp=y_peer)

    sends_up = jnp.logical_and(z >= sp, z < n_z - 1)
    sends_down = jnp.logical_and(z <= sp, z > 0)

    def w_send(c):
        @pl.when(sends_up)
        def _():
            wz_copy(0, c, z + 1).start()

        @pl.when(sends_down)
        def _():
            wz_copy(1, c, z - 1).start()

    def w_cross(c):
        wy_copy(y, c).start()

    near = z // PAIR == x
    far = z // PAIR != x
    held = w_chunks - 2

    @pl.when(z == sp)
    def _():
        w_load.wait()
        for c in range(w_chunks):
            w_send(c)
        x_start()
        for c in range(held):
            w_cross(c)

    @pl.when(z != sp)
    def _():
        x_start()

    def w_step(c, cross=True):
        @pl.when(z != sp)
        def _():
            wz_copy(0, c, z).wait_recv()
            w_send(c)
            if cross:
                w_cross(c)

    lane = lax.broadcasted_iota(jnp.int32, (1, LANES), 1)

    def head_mask(sub):
        return lane // head_width == sub

    def pair_cols(pair):
        return pl.ds(pl.multiple_of(pair * LANES, LANES), LANES)

    for load in loads[1:4]:
        load.wait()
    cum = cum_ref[...]
    cum_cols = jnp.concatenate([cum] * (-(-8 // n_heads)), axis=0).T

    def masked_query(pair, sub):
        return jnp.where(head_mask(sub), q_ref[:, pair_cols(pair)], 0)

    def probabilities(h):
        keys = k_ref[:, pair_cols(h // per_pair)]
        query = masked_query(h // per_pair, h % per_pair)
        for b in range(n_blocks):
            lo, end = b * block, (b + 1) * block
            scores = nt(keys[:end], query[lo:end]) * scale
            scores = scores + cum[h:h + 1, lo:end] - cum_cols[:end, h:h + 1]
            key_pos = lax.broadcasted_iota(jnp.int32, (end, block), 0)
            query_pos = lo + lax.broadcasted_iota(jnp.int32, (end, block), 1)
            scores = jnp.where(key_pos <= query_pos, scores, -1e30)
            weights = jnp.exp(scores - jnp.max(scores, axis=0, keepdims=True))
            weights = weights * (1.0 / jnp.sum(weights, axis=0, keepdims=True))
            prob[h, :end, lo:end] = weights
            prob_b[h, :end, lo:end] = weights.astype(jnp.bfloat16)

    def key_transpose():
        k_t[...] = k_ref[...].T

    def output_transpose():
        loads[4].wait()
        loads[5].wait()
        o_t[...] = o_ref[...].T

    step_of = jnp.where(x == 0, z, n_z - 1 - z)

    def dp_at(step, lane_y):
        return jnp.where(x == 0, step, n_z - 1 - step) * PAIR + lane_y

    def lane_of(other):
        return 1 - y if other else y

    def product(step, other):
        row = pl.multiple_of(dp_at(step, lane_of(other)) * w_rows, w_rows)
        return nn(o_t[pl.ds(row, w_rows), :], dof[:, col_at(sp)])

    def keep(step, other):
        dw_part[2 * step + other] = product(step, other)

    def y_copy(slot):
        return remote(y_send.at[slot], y_recv.at[slot], ry_ssem, ry_rsem.at[slot],
                      sp=sp, dp=y_peer)

    def z_copy(source, target, step):
        return remote(z_send.at[source], z_recv.at[target], rz_ssem, rz_rsem.at[target],
                      sp=sp, dp=dp_at(step, y))

    def to_y(slot, value):
        y_send[slot] = value.astype(jnp.bfloat16)
        y_copy(slot).start()

    def to_z(source, value, target, step):
        z_send[source] = value.astype(jnp.bfloat16)
        z_copy(source, target, step).start()

    def from_y(slot):
        y_copy(slot).wait_recv()
        return y_recv[slot].astype(jnp.float32)

    def from_z(target):
        z_copy(0, target, step_of).wait_recv()
        return z_recv[target].astype(jnp.float32)

    def part_of(step, other):
        return dw_part[2 * step + other]

    def columns_arrive():
        forward_copy(0, 1 - core).wait_recv()
        first = pl.multiple_of((1 - x) * PAIR * col_part, PAIR * col_part)
        part = dof.at[token_rows((1 - x) * PAIR + 1 - core), pl.ds(first, PAIR * col_part)]
        remote(part, part, f_ssem, f_rsem.at[1], sp=core_peer, dp=dp).wait_recv()

    outs = (dq_out, dk_out, dv_out)

    def grad_cols(pair):
        return pl.ds(pl.multiple_of(sp * head_cols + pair * LANES, LANES), LANES)

    def pair_of(turn):
        return y if turn == 0 else 1 - y

    def grad_copy(a, turn, off):
        target = (sp + off) % n_sp
        pair = pair_of(turn)
        return remote(stage.at[a, token_rows(target), pair_cols(pair)],
                      outs[a].at[0, :, grad_cols(pair)],
                      g_ssem, g_rsem, sp=target, dp=dp)

    def grad_keep(a, turn):
        pair = pair_of(turn)
        return pltpu.make_async_copy(stage.at[a, token_rows(sp), pair_cols(pair)],
                                     outs[a].at[0, :, grad_cols(pair)], g_lsem)

    def add_rows(totals, part):
        for b in range(part.shape[0] // block):
            piece = part[b * block:(b + 1) * block]
            totals[b] = piece if totals[b] is None else totals[b] + piece

    def send_grad(a, turn):
        for off in range(1, n_sp):
            grad_copy(a, turn, off).start()
        grad_keep(a, turn).start()

    def picked(left, pick):
        high = left.astype(jnp.bfloat16)
        low = (left - high.astype(jnp.float32)).astype(jnp.bfloat16)
        row = lax.broadcasted_iota(jnp.int32, (8, 2 * LANES), 0)
        column = lax.broadcasted_iota(jnp.int32, (8, 2 * LANES), 1) % LANES
        picks = jnp.where(pick(row, column), 1.0, 0.0).astype(jnp.bfloat16)
        return nt(picks, jnp.concatenate([high, low], axis=1))

    def pair_gradients(turn, early, between):
        pair = pair_of(turn)
        cols = pair_cols(pair)
        if turn:
            block_w = wbuf.at[pl.ds(pl.multiple_of((1 - y) * w_rows, w_rows), w_rows)]
            remote(block_w, block_w, wy_ssem, wy_rsem, sp=sp, dp=y_peer).wait_recv()
        with ns(f"pair{turn}a0"):
            pair_w = wbuf[pl.ds(pl.multiple_of(pair * w_rows, w_rows), w_rows), :]
            cot = nt(dof[...], pair_w).astype(jnp.bfloat16)
            cots = [jnp.where(head_mask(sub), cot, 0) for sub in range(per_pair)]
        with ns(f"pair{turn}a1"):
            value_total = [None] * n_blocks
            for sub in range(per_pair):
                h = pair * per_pair + sub
                for b in range(n_blocks):
                    lo, end = b * block, (b + 1) * block
                    add_rows(value_total, nn(prob_b[h, :end, lo:end], cots[sub][lo:end]))
            stage[2, :, cols] = jnp.concatenate(value_total, axis=0).astype(jnp.bfloat16)
            send_grad(2, turn)
        early()
        with ns(f"pair{turn}a2"):
            own_out = o_ref[:, grad_cols(pair)]
            values = v_ref[:, cols]
            dots = picked(cot.astype(jnp.float32) * own_out.astype(jnp.float32),
                          lambda row, column: column // head_width == row)
        key_totals, query_total, row_sums = [], [], []
        for sub in range(per_pair):
            with ns(f"pair{turn}b{sub}"):
                h = pair * per_pair + sub
                spare = jnp.where(lane == (1 - sub) * head_width, 1.0, 0.0).astype(jnp.bfloat16)
                query_h = jnp.where(head_mask(sub), q_ref[:, cols], spare)
                keys_t = k_t[pl.ds(pl.multiple_of(h * head_width, head_width), head_width), :]
                keys_t = jnp.concatenate([keys_t, jnp.ones((16, length), jnp.bfloat16)], axis=0)
                key_total, query_parts = [None] * n_blocks, []
                for b in range(n_blocks):
                    lo, end = b * block, (b + 1) * block
                    weights = prob[h, :end, lo:end]
                    d_prob = nt(values[:end], cots[sub][lo:end])
                    score_b = (weights * (d_prob - dots[sub:sub + 1, lo:end])).astype(jnp.bfloat16)
                    add_rows(key_total, nn(score_b, query_h[lo:end]))
                    query_parts.append(nn(keys_t[:, :end], score_b))
                key_totals.append(jnp.concatenate(key_total, axis=0))
                query_sums = jnp.concatenate(query_parts, axis=1)
                query_total.append(query_sums[:head_width])
                row_sums.append(query_sums[head_width:head_width + 1])
            if sub == 0:
                between()
        with ns(f"pair{turn}c"):
            first = head_mask(0)
            key_grad = jnp.where(first, key_totals[0], key_totals[1])
            stage[1, :, cols] = (key_grad * scale).astype(jnp.bfloat16)
            send_grad(1, turn)
            stage[0, :, cols] = (jnp.concatenate(query_total, axis=0).T * scale).astype(jnp.bfloat16)
            send_grad(0, turn)
            col_sums = picked(jnp.where(first, key_totals[1], key_totals[0]),
                              lambda row, column: column == (1 - row) * head_width)
            for sub in range(per_pair):
                d_cum = row_sums[sub] - col_sums[sub:sub + 1]
                dcum_ref[pl.ds(pair * per_pair + sub, 1), :] = d_cum

    def at_step(step):
        return lambda action: pl.when(step_of == step)(action)

    with ns("a_prep"):
        output_transpose()
        key_transpose()
        core_copy(sp).start()
        for h in range(n_heads):
            probabilities(h)

    def relay(first, last):
        for c in range(first, last):
            w_step(c)

    def columns_first(ahead):
        lax.fori_loop(0, ahead, lambda c, done: (w_step(c), done)[1], 0)
        forward_step(0)

        core_copy(core_peer).wait_recv()

    def w_later(c, ahead):
        @pl.when(c >= ahead)
        def _():
            w_step(c)

    def relay2(first, last):
        for c in range(first, last):
            w_later(c, ahead2)

    def relay3(first, last):
        for c in range(first, last):
            w_later(c, ahead3)

    def far_near(n):
        step, other = n % 2, 1 - n // 2
        value = product(step, other)

        @at_step(3)
        def _():
            to_z(n, value, n, 2)

        @at_step(2)
        def _():
            dw_part[2 * step + other] = value

    def far_cross(slot, step):
        y_send[slot] = product(step, 1).astype(jnp.bfloat16)

    ahead2 = jnp.where(x == 0, core * w_chunks, 2)
    ahead3 = jnp.where(x == 0, core * w_chunks, 0)

    with ns("b_relay"):
        @pl.when(near)
        def _():
            relay(0, 4)

            @pl.when(core == 0)
            def _():
                forward_step(0)

            for c in range(4, w_chunks):
                w_step(c, c < held)

            @pl.when(core == 1)
            def _():
                forward_step(0)

            core_copy(core_peer).wait_recv()

        @at_step(2)
        def _():
            columns_first(ahead2)

        @at_step(3)
        def _():
            columns_first(ahead3)

    with ns("d_dw"):
        @pl.when(near)
        def _():
            sibling = 1 - step_of
            to_y(0, product(3, 1))
            to_y(1, product(2, 1))
            for c in range(held, w_chunks):
                w_cross(c)
            to_z(0, product(sibling, 1), 2, sibling)
            to_z(1, product(sibling, 0), 3, sibling)
            keep(3, 0)
            forward_step(1)
            keep(2, 0)
            keep(step_of, 1)
            keep(step_of, 0)
            forward_step(2)

        @at_step(2)
        def _():
            relay2(0, 1)
            far_near(0)
            relay2(1, 2)
            far_near(1)
            relay2(2, 3)
            far_near(2)
            relay2(3, 4)
            far_near(3)
            relay2(4, 5)
            far_cross(0, 3)
            relay2(5, 6)
            far_cross(1, 2)
            relay2(6, 7)
            keep(3, 0)
            relay2(7, 8)
            forward_step(1)
            y_copy(0).start()
            y_copy(1).start()
            keep(2, 0)
            forward_step(2)

        @at_step(3)
        def _():
            for n in range(4):
                far_near(n)

            relay3(0, 2)
            far_cross(0, 2)

            @pl.when(x == 0)
            def _():
                forward_step(1)

            relay3(2, 4)
            far_cross(1, 3)

            @pl.when(x == 0)
            def _():
                forward_step(2)

            relay3(4, 6)
            keep(2, 0)

            @pl.when(x == 1)
            def _():
                forward_step(1)
                forward_step(2)

            keep(3, 0)
            relay3(6, 8)
            y_copy(0).start()
            y_copy(1).start()

    with ns("e_cols2"):
        columns_arrive()

    def pass_on(n):
        step, other = n % 2, 1 - n // 2
        to_z(n, part_of(step, other) + from_z(n), 1 - other, step)

    def near_far(slot, step):
        return part_of(step, 0) + from_y(slot)

    def over_y():
        to_y(2, part_of(step_of, 1) + from_z(0) + from_z(2))

    with ns("f_poll"):
        @at_step(0)
        def _():
            to_z(2, near_far(0, 3), 4, 1)

        @at_step(1)
        def _():
            dw_part[6] = near_far(0, 3)

        @at_step(2)
        def _():
            pass_on(0)

    def between0():
        with ns("g_poll"):
            @at_step(0)
            def _():
                to_z(3, near_far(1, 2), 5, 2)

            @at_step(1)
            def _():
                to_z(3, near_far(1, 2), 6, 2)

            @at_step(2)
            def _():
                pass_on(1)

    pair_gradients(0, lambda: None, between0)
    with ns("h_poll"):
        @at_step(2)
        def _():
            pass_on(2)
            pass_on(3)

    def early1():
        with ns("i0_poll"):
            @at_step(3)
            def _():
                to_z(4, part_of(2, 0) + from_y(0), 4, 2)

    def between1():
        with ns("i_poll"):
            @at_step(0)
            def _():
                over_y()

            @at_step(1)
            def _():
                to_z(2, part_of(3, 0) + from_z(4), 5, 3)

            @at_step(2)
            def _():
                to_z(4, part_of(3, 0) + from_y(0), 4, 3)

    pair_gradients(1, early1, between1)
    with ns("j_poll"):
        @at_step(1)
        def _():
            over_y()

    with ns("k_final"):
        @pl.when(near)
        def _():
            dw_acc[...] = part_of(step_of, 0) + from_z(1) + from_z(3) + from_y(2)

        @at_step(2)
        def _():
            dw_acc[...] = part_of(2, 0) + from_y(1) + from_z(5) + from_z(6) + from_z(4)

        @at_step(3)
        def _():
            dw_acc[...] = part_of(3, 0) + from_y(1) + from_z(4) + from_z(5)

    results = [
        pltpu.make_async_copy(dw_acc, dw_out, out_sem.at[0]),
        pltpu.make_async_copy(dcum_ref, dcum_out.at[0], out_sem.at[1]),
    ]
    for result in results:
        result.start()

    def sent(part, sem):
        remote(part, part, sem, sem, sp=core_peer, dp=dp).wait_send()

    own_rows = dof.at[token_rows(sp)]
    block_w = wbuf.at[own_w]
    rest = stage.at[:, pl.ds(0, length - tokens)]
    with ns("o_waitsend"):
        sent(own_rows, x_ssem)
        sent(own_rows, f_ssem)
        core_copy(sp).wait_send()
        sent(block_w, wy_ssem)

        @pl.when(sends_up)
        def _():
            sent(block_w, wz_ssem.at[0])

        @pl.when(sends_down)
        def _():
            sent(block_w, wz_ssem.at[1])

        @pl.when(near)
        def _():
            sent(y_send, ry_ssem)
            sent(z_send.at[pl.ds(0, 4)], rz_ssem)

        @pl.when(far)
        def _():
            sent(y_send.at[pl.ds(0, 2)], ry_ssem)
            sent(z_send, rz_ssem)

        sent(rest, g_ssem)
    with ns("p_gradwait"):
        remote(rest, rest, g_ssem, g_rsem, sp=core_peer, dp=dp).wait_recv()
        kept = stage.at[:, pl.ds(0, tokens)]
        pltpu.make_async_copy(kept, kept, g_lsem).wait()
    with ns("q_results"):
        for result in results:
            result.wait()


def hand_over(*refs):
    count = len(refs) // 2
    copies = [
        pltpu.make_async_copy(refs[i], refs[count + i], refs[-1].at[i]) for i in range(count)
    ]
    for copy in copies:
        copy.start()
    for copy in copies:
        copy.wait()


def fits(mesh, query, cum, d_out, w_out):
    n_sp, n_dp = mesh.shape["sp"], mesh.shape["dp"]
    head_cols, n_heads = query.shape[2] // n_sp, cum.shape[1] // n_sp
    length, width = d_out.shape[1], d_out.shape[2]
    w_rows = w_out.shape[0] // n_dp
    if head_cols % LANES or n_heads == 0 or 8 % n_heads:
        return False
    if LANES != PAIR * (head_cols // n_heads) or length % (2 * LANES) or (width // n_sp) % LANES:
        return False
    if n_sp & (n_sp - 1) or n_sp < PAIR or n_dp != PAIR * n_sp or n_sp != PAIR * PAIR or head_cols != PAIR * LANES or w_rows != LANES:
        return False
    held = 6 * n_heads * length**2 + 2 * length * width + 8 * length * query.shape[2]
    return held < 32 * 2**20


def fused_shards(n_sp, n_dp, query, keys, values, output, cum, d_out, w_out):
    arrays = (query, keys, values, output, cum, d_out, w_out)
    length, head_cols = query.shape[1:]
    attn = output.shape[2]
    n_heads = cum.shape[1]
    tokens, width = d_out.shape[1:]
    w_rows = w_out.shape[0]
    n_z, col_part = n_dp // PAIR, width // n_sp
    w_chunks = 8
    bf16, f32 = jnp.bfloat16, jnp.float32
    dma = pltpu.SemaphoreType.DMA
    n_pairs = head_cols // LANES
    anywhere = pl.BlockSpec(memory_space=pl.ANY)
    from_hbm = pl.BlockSpec(memory_space=pltpu.HBM)
    grad = jax.ShapeDtypeStruct((1, tokens, attn), bf16)
    found = pl.pallas_call(
        functools.partial(kernel, n_sp, n_dp, n_heads, w_chunks),
        out_shape=(
            grad, grad, grad,
            jax.ShapeDtypeStruct(cum.shape, f32),
            jax.ShapeDtypeStruct((w_rows, col_part), f32),
        ),
        in_specs=[from_hbm] * 7,
        out_specs=[anywhere] * 5,
        scratch_shapes=[
            pltpu.VMEM((length, head_cols), bf16),
            pltpu.VMEM((length, head_cols), bf16),
            pltpu.VMEM((length, head_cols), bf16),
            pltpu.VMEM((length, attn), bf16),
            pltpu.VMEM(cum.shape[1:], f32),
            pltpu.VMEM((length, width), bf16),
            pltpu.VMEM((PAIR * w_rows, width), bf16),
            pltpu.VMEM((n_heads, length, length), f32),
            pltpu.VMEM((n_heads, length, length), bf16),
            pltpu.VMEM((head_cols, length), bf16),
            pltpu.VMEM((attn, length), bf16),
            pltpu.VMEM((PAIR * n_z, w_rows, col_part), f32),
            pltpu.VMEM((3, w_rows, col_part), bf16),
            pltpu.VMEM((3, w_rows, col_part), bf16),
            pltpu.VMEM((5, w_rows, col_part), bf16),
            pltpu.VMEM((7, w_rows, col_part), bf16),
            pltpu.VMEM((w_rows, col_part), f32),
            pltpu.VMEM((3, length, head_cols), bf16),
            pltpu.VMEM(cum.shape[1:], f32),
            dma((7,)), dma((2,)),
            dma, dma((n_sp - 1,)), dma, dma, dma, dma((PAIR,)),
            dma((2,)), dma((w_chunks,)), dma, dma,
            dma, dma((3,)), dma, dma((7,)),
            dma, dma, dma,
        ],
        compiler_params=pltpu.CompilerParams(
            collective_id=0, has_side_effects=True, vmem_limit_bytes=48 * 2**20
        ),
    )(*[pltpu.with_memory_space_constraint(array, pltpu.HBM) for array in arrays])
    return pl.pallas_call(
        hand_over,
        out_shape=[jax.ShapeDtypeStruct(part.shape, part.dtype) for part in found],
        in_specs=[anywhere] * len(found),
        out_specs=[from_hbm] * len(found),
        scratch_shapes=[dma((len(found),))],
        compiler_params=pltpu.CompilerParams(vmem_limit_bytes=2**20),
    )(*found)


def solution(mesh):
    n_sp, n_dp = mesh.shape["sp"], mesh.shape["dp"]
    placed = (
        P("dp", None, "sp"), P("dp", None, "sp"), P("dp", None, "sp"), P("dp", None, None),
        P("dp", "sp", None), P("dp", "sp", None), P("dp", None),
    )
    results = (
        P("dp", "sp", None), P("dp", "sp", None), P("dp", "sp", None), P("dp", "sp", None),
        P("dp", "sp"),
    )

    def run(query, keys, values, output, cum, d_out, w_out):
        if fits(mesh, query, cum, d_out, w_out):
            body = functools.partial(fused_shards, n_sp, n_dp)
            step = jax.shard_map(
                body, mesh=mesh, in_specs=placed, out_specs=results, check_vma=False
            )
        else:
            step = plain_solution(mesh)
        return step(query, keys, values, output, cum, d_out, w_out)

    return run
```

```python
import contextlib
import functools

import jax
import jax.numpy as jnp
from jax import lax
from jax.experimental import pallas as pl
from jax.experimental.pallas import tpu as pltpu
from jax.sharding import PartitionSpec as P


def head_grads(query, keys, values, output, cotangent, cum):
    head_count, length, head_width = query.shape
    span_rows = min(512, length)
    score_scale = head_width ** (-0.5)
    row_dots = jnp.sum(cotangent.astype(jnp.float32) * output.astype(jnp.float32), axis=2)
    positions = jnp.arange(length)

    def product(left, right, form):
        return jnp.einsum(form, left, right, preferred_element_type=jnp.float32)

    def advance(totals, block_index):
        key_grad, value_grad, cum_grad = totals
        offset = block_index * span_rows
        query_blk = lax.dynamic_slice_in_dim(query, offset, span_rows, 1)
        cot_blk = lax.dynamic_slice_in_dim(cotangent, offset, span_rows, 1)
        cum_blk = lax.dynamic_slice_in_dim(cum, offset, span_rows, 1)
        dots_blk = lax.dynamic_slice_in_dim(row_dots, offset, span_rows, 1)
        scores = product(query_blk, keys, "hqe,hke->hqk") * score_scale
        scores = scores + cum_blk[:, :, None] - cum[:, None, :]
        query_pos = offset + jnp.arange(span_rows)
        causal = positions[None, :] <= query_pos[:, None]
        scores = jnp.where(causal[None], scores, -1e30)
        row_max = jnp.max(scores, axis=2, keepdims=True)
        weights = jnp.exp(scores - row_max)
        weights = weights / jnp.sum(weights, axis=2, keepdims=True)
        weights_b = weights.astype(jnp.bfloat16)
        d_prob = product(cot_blk, values, "hqe,hke->hqk")
        d_score = weights * (d_prob - dots_blk[:, :, None])
        score_b = d_score.astype(jnp.bfloat16)
        query_grad = (product(score_b, keys, "hqk,hke->hqe") * score_scale).astype(jnp.bfloat16)
        key_grad = key_grad + product(score_b, query_blk, "hqk,hqe->hke") * score_scale
        value_grad = value_grad + product(weights_b, cot_blk, "hqk,hqe->hke")
        cum_grad = cum_grad - jnp.sum(d_score, axis=1)
        own_part = lax.dynamic_slice_in_dim(cum_grad, offset, span_rows, 1) + jnp.sum(
            d_score, axis=2
        )
        cum_grad = lax.dynamic_update_slice_in_dim(cum_grad, own_part, offset, 1)
        return ((key_grad, value_grad, cum_grad), query_grad)

    start_state = (
        jnp.zeros(query.shape, jnp.float32),
        jnp.zeros(query.shape, jnp.float32),
        jnp.zeros(cum.shape, jnp.float32),
    )
    totals, query_blocks = lax.scan(advance, start_state, jnp.arange(length // span_rows))
    query_grad = jnp.transpose(query_blocks, (1, 0, 2, 3)).reshape(query.shape)
    return (query_grad, totals[0].astype(jnp.bfloat16), totals[1].astype(jnp.bfloat16), totals[2])


def shards(query, keys, values, output, cum, d_out, w_out):
    local_rows = d_out[0]
    whole_output = output[0]
    d_attn = lax.dot_general(
        local_rows,
        lax.all_gather(w_out, "dp", axis=0, tiled=True),
        (((1,), (1,)), ((), ())),
        preferred_element_type=jnp.float32,
    ).astype(jnp.bfloat16)
    head_cot, column_part = (
        lax.all_to_all(d_attn[None], "sp", split_axis=2, concat_axis=1, tiled=True),
        lax.all_to_all(d_out, "sp", split_axis=2, concat_axis=1, tiled=True),
    )
    grad_weight = lax.psum_scatter(
        lax.dot_general(
            whole_output,
            column_part[0],
            (((0,), (0,)), ((), ())),
            preferred_element_type=jnp.float32,
        ),
        "dp",
        scatter_dimension=0,
        tiled=True,
    )
    head_cols = query.shape[2]
    head_count = cum.shape[1]
    head_width = head_cols // head_count
    seq_length = query.shape[1]
    own_output = lax.dynamic_slice_in_dim(
        whole_output, lax.axis_index("sp") * head_cols, head_cols, 1
    )

    def heads_first(matrix):
        return jnp.transpose(matrix.reshape(seq_length, head_count, head_width), (1, 0, 2))

    def tokens_first(matrix):
        return jnp.transpose(matrix, (1, 0, 2)).reshape(1, seq_length, head_cols)

    grads = head_grads(
        heads_first(query[0]),
        heads_first(keys[0]),
        heads_first(values[0]),
        heads_first(own_output),
        heads_first(head_cot[0]),
        cum[0],
    )
    query_grad, key_grad, value_grad = (
        lax.all_to_all(tokens_first(grads[0]), "sp", split_axis=1, concat_axis=2, tiled=True),
        lax.all_to_all(tokens_first(grads[1]), "sp", split_axis=1, concat_axis=2, tiled=True),
        lax.all_to_all(tokens_first(grads[2]), "sp", split_axis=1, concat_axis=2, tiled=True),
    )
    return (query_grad, key_grad, value_grad, grads[3][None], grad_weight)


def plain_solution(mesh):
    placed = (
        P("dp", None, "sp"),
        P("dp", None, "sp"),
        P("dp", None, "sp"),
        P("dp", None, None),
        P("dp", "sp", None),
        P("dp", "sp", None),
        P("dp", None),
    )
    return jax.shard_map(
        shards,
        mesh=mesh,
        in_specs=placed,
        out_specs=(
            P("dp", "sp", None),
            P("dp", "sp", None),
            P("dp", "sp", None),
            P("dp", "sp", None),
            P("dp", "sp"),
        ),
        check_vma=False,
    )


MESH = pl.DeviceIdType.MESH
ns = contextlib.nullcontext
PAIR = 2
LANES = 128


def nt(left, right):
    return lax.dot_general(
        left, right, (((1,), (1,)), ((), ())), preferred_element_type=jnp.float32
    )


def nn(left, right):
    return lax.dot_general(
        left, right, (((1,), (0,)), ((), ())), preferred_element_type=jnp.float32
    )


def kernel(
    n_sp, n_dp, n_heads, w_chunks,
    q_hbm, k_hbm, v_hbm, o_hbm, cum_hbm, do_hbm, w_hbm,
    dq_out, dk_out, dv_out, dcum_out, dw_out,
    q_ref, k_ref, v_ref, o_ref, cum_ref, dof, wbuf, prob, prob_b, k_t, o_t,
    dw_part, y_send, y_recv, z_send, z_recv, dw_acc, cot_acc, stage, dcum_ref,
    in_sem, out_sem,
    x_ssem, x_rsem, c_ssem, c_rsem, f_ssem, f_rsem,
    wz_ssem, wz_rsem, wy_ssem, wy_rsem,
    ry_ssem, ry_rsem, rz_ssem, rz_rsem,
    g_ssem, g_rsem, g_lsem,
):
    sp, dp = lax.axis_index("sp"), lax.axis_index("dp")
    n_z = n_dp // PAIR
    x, core = sp // PAIR, sp % PAIR
    z, y = dp // PAIR, dp % PAIR
    length, head_cols = q_ref.shape
    head_width = head_cols // n_heads
    tokens, width = do_hbm.shape[1:]
    w_rows = w_hbm.shape[0]
    col_part = width // n_sp
    scale = head_width ** (-0.5)
    per_pair = LANES // head_width
    n_pairs = head_cols // LANES
    block = min(2 * LANES, length)
    n_blocks = length // block
    core_peer = x * PAIR + (1 - core)
    y_peer = z * PAIR + (1 - y)

    def token_rows(owner):
        return pl.ds(pl.multiple_of(owner * tokens, tokens), tokens)

    def col_at(part):
        return pl.ds(pl.multiple_of(part * col_part, LANES), col_part)

    def remote(src, dst, ssem, rsem, **where):
        return pltpu.make_async_remote_copy(
            src_ref=src, dst_ref=dst, send_sem=ssem, recv_sem=rsem,
            device_id=where, device_id_type=MESH,
        )

    own_w = pl.ds(pl.multiple_of(y * w_rows, w_rows), w_rows)
    loads = [
        pltpu.make_async_copy(do_hbm.at[0], dof.at[token_rows(sp)], in_sem.at[0]),
        pltpu.make_async_copy(q_hbm.at[0], q_ref, in_sem.at[2]),
        pltpu.make_async_copy(k_hbm.at[0], k_ref, in_sem.at[3]),
        pltpu.make_async_copy(cum_hbm.at[0], cum_ref, in_sem.at[4]),
        pltpu.make_async_copy(v_hbm.at[0], v_ref, in_sem.at[5]),
        pltpu.make_async_copy(o_hbm.at[0], o_ref, in_sem.at[6]),
    ]
    w_load = pltpu.make_async_copy(w_hbm, wbuf.at[own_w], in_sem.at[1])
    loads[0].start()

    @pl.when(z == sp)
    def _():
        w_load.start()

    for load in loads[1:]:
        load.start()

    barrier = pltpu.get_barrier_semaphore()
    for off in range(1, n_sp):
        pl.semaphore_signal(
            barrier, inc=1, device_id={"sp": (sp + off) % n_sp, "dp": dp}, device_id_type=MESH
        )
    for off in range(1, n_z):
        pl.semaphore_signal(
            barrier, inc=1,
            device_id={"sp": sp, "dp": ((z + off) % n_z) * PAIR + y}, device_id_type=MESH,
        )
    pl.semaphore_signal(barrier, inc=1, device_id={"sp": sp, "dp": y_peer}, device_id_type=MESH)
    pl.semaphore_wait(barrier, n_sp + n_z - 1)

    def chip_rows(owner_x):
        return pl.ds(pl.multiple_of(owner_x * PAIR * tokens, PAIR * tokens), PAIR * tokens)

    def x_out(i):
        part = dof.at[token_rows(sp), col_at(((1 - x) * PAIR + i) % n_sp)]
        slot, target_core = (0, i) if i < PAIR else (i - 1, core)
        return remote(part, part, x_ssem, x_rsem.at[slot], sp=(1 - x) * PAIR + target_core, dp=dp)

    def arrived(i, owner_core):
        if i == 0:
            return dof.at[chip_rows(1 - x), col_at(x * PAIR + owner_core)]
        owner = (1 - x) * PAIR + owner_core
        return dof.at[token_rows(owner), col_at((x * PAIR + i + 1) % n_sp)]

    def x_in(i):
        part = arrived(i, core)
        return remote(part, part, x_ssem, x_rsem.at[i], sp=core_peer, dp=dp)

    def core_copy(owner):
        part = dof.at[token_rows(owner)]
        return remote(part, part, c_ssem, c_rsem, sp=core_peer, dp=dp)

    def forward_copy(i, owner_core):
        part = arrived(i, owner_core)
        return remote(part, part, f_ssem, f_rsem.at[i], sp=core_peer, dp=dp)

    def x_start():
        loads[0].wait()
        for i in range(n_sp):
            x_out(i).start()

    def forward_step(i):
        x_in(i).wait_recv()
        forward_copy(i, core).start()

    chunk_cols = width // w_chunks

    def w_part(owner_y, c):
        rows = pl.ds(pl.multiple_of(owner_y * w_rows, w_rows), w_rows)
        start = (x * (w_chunks // PAIR) + c) % w_chunks * chunk_cols
        return wbuf.at[rows, pl.ds(pl.multiple_of(start, chunk_cols), chunk_cols)]

    def wz_copy(way, c, target_z):
        return remote(w_part(y, c), w_part(y, c), wz_ssem.at[way], wz_rsem.at[c],
                      sp=sp, dp=target_z * PAIR + y)

    def w_group(c):
        quarter = c * n_sp // w_chunks
        return max(quarter - 1, 0) if isinstance(c, int) else jnp.maximum(quarter - 1, 0)

    def wy_copy(owner_y, c):
        return remote(w_part(owner_y, c), w_part(owner_y, c), wy_ssem, wy_rsem.at[w_group(c)],
                      sp=sp, dp=y_peer)

    sends_up = jnp.logical_and(z >= sp, z < n_z - 1)
    sends_down = jnp.logical_and(z <= sp, z > 0)

    def w_send(c):
        @pl.when(sends_up)
        def _():
            wz_copy(0, c, z + 1).start()

        @pl.when(sends_down)
        def _():
            wz_copy(1, c, z - 1).start()

    def w_cross(c):
        wy_copy(y, c).start()

    near = z // PAIR == x
    far = z // PAIR != x
    held = w_chunks - 2

    @pl.when(z == sp)
    def _():
        w_load.wait()
        for c in range(w_chunks):
            w_send(c)
        x_start()
        for c in range(held):
            w_cross(c)

    @pl.when(z != sp)
    def _():
        x_start()

    def w_step(c, cross=True):
        @pl.when(z != sp)
        def _():
            wz_copy(0, c, z).wait_recv()
            w_send(c)
            if cross:
                w_cross(c)

    lane = lax.broadcasted_iota(jnp.int32, (1, LANES), 1)

    def head_mask(sub):
        return lane // head_width == sub

    def pair_cols(pair):
        return pl.ds(pl.multiple_of(pair * LANES, LANES), LANES)

    for load in loads[1:4]:
        load.wait()
    cum = cum_ref[...]
    cum_cols = jnp.concatenate([cum] * (-(-8 // n_heads)), axis=0).T

    def masked_query(pair, sub):
        return jnp.where(head_mask(sub), q_ref[:, pair_cols(pair)], 0)

    def probabilities(h):
        keys = k_ref[:, pair_cols(h // per_pair)]
        query = masked_query(h // per_pair, h % per_pair)
        for b in range(n_blocks):
            lo, end = b * block, (b + 1) * block
            scores = nt(keys[:end], query[lo:end]) * scale
            scores = scores + cum[h:h + 1, lo:end] - cum_cols[:end, h:h + 1]
            key_pos = lax.broadcasted_iota(jnp.int32, (end, block), 0)
            query_pos = lo + lax.broadcasted_iota(jnp.int32, (end, block), 1)
            scores = jnp.where(key_pos <= query_pos, scores, -1e30)
            weights = jnp.exp(scores - jnp.max(scores, axis=0, keepdims=True))
            weights = weights * (1.0 / jnp.sum(weights, axis=0, keepdims=True))
            prob[h, :end, lo:end] = weights
            prob_b[h, :end, lo:end] = weights.astype(jnp.bfloat16)

    def key_transpose():
        k_t[...] = k_ref[...].T

    def output_transpose():
        loads[4].wait()
        loads[5].wait()
        o_t[...] = o_ref[...].T

    step_of = jnp.where(x == 0, z, n_z - 1 - z)

    def dp_at(step, lane_y):
        return jnp.where(x == 0, step, n_z - 1 - step) * PAIR + lane_y

    def lane_of(other):
        return 1 - y if other else y

    def product(step, other):
        row = pl.multiple_of(dp_at(step, lane_of(other)) * w_rows, w_rows)
        return nn(o_t[pl.ds(row, w_rows), :], dof[:, col_at(sp)])

    def keep(step, other):
        dw_part[2 * step + other] = product(step, other)

    def y_copy(slot):
        return remote(y_send.at[slot], y_recv.at[slot], ry_ssem, ry_rsem.at[slot],
                      sp=sp, dp=y_peer)

    def z_copy(source, target, step):
        return remote(z_send.at[source], z_recv.at[target], rz_ssem, rz_rsem.at[target],
                      sp=sp, dp=dp_at(step, y))

    def to_y(slot, value):
        y_send[slot] = value.astype(jnp.bfloat16)
        y_copy(slot).start()

    def to_z(source, value, target, step):
        z_send[source] = value.astype(jnp.bfloat16)
        z_copy(source, target, step).start()

    def from_y(slot):
        y_copy(slot).wait_recv()
        return y_recv[slot].astype(jnp.float32)

    def from_z(target):
        z_copy(0, target, step_of).wait_recv()
        return z_recv[target].astype(jnp.float32)

    def part_of(step, other):
        return dw_part[2 * step + other]

    def pair_of(turn):
        return y if turn == 0 else 1 - y

    def columns_arrive(i):
        forward_copy(i, 1 - core).wait_recv()

    def cot_piece(pair, first, count):
        start = pl.multiple_of((x * PAIR + first) % n_sp * col_part, col_part)
        cols = pl.ds(start, count * col_part)
        return nt(dof[:, cols], wbuf[pl.ds(pl.multiple_of(pair * w_rows, w_rows), w_rows), cols])

    def cot_first():
        columns_arrive(0)
        cot_acc[...] = cot_piece(pair_of(0), 0, PAIR)

    def cot_second():
        columns_arrive(1)
        cot_acc[...] += cot_piece(pair_of(0), PAIR, 1)

    outs = (dq_out, dk_out, dv_out)

    def grad_cols(pair):
        return pl.ds(pl.multiple_of(sp * head_cols + pair * LANES, LANES), LANES)

    def grad_copy(a, turn, off):
        target = (sp + off) % n_sp
        pair = pair_of(turn)
        return remote(stage.at[a, token_rows(target), pair_cols(pair)],
                      outs[a].at[0, :, grad_cols(pair)],
                      g_ssem, g_rsem, sp=target, dp=dp)

    def grad_keep(a, turn):
        pair = pair_of(turn)
        return pltpu.make_async_copy(stage.at[a, token_rows(sp), pair_cols(pair)],
                                     outs[a].at[0, :, grad_cols(pair)], g_lsem)

    def add_rows(totals, part):
        for b in range(part.shape[0] // block):
            piece = part[b * block:(b + 1) * block]
            totals[b] = piece if totals[b] is None else totals[b] + piece

    def send_grad(a, turn):
        for off in range(1, n_sp):
            grad_copy(a, turn, off).start()
        grad_keep(a, turn).start()

    def picked(left, pick):
        high = left.astype(jnp.bfloat16)
        low = (left - high.astype(jnp.float32)).astype(jnp.bfloat16)
        row = lax.broadcasted_iota(jnp.int32, (8, 2 * LANES), 0)
        column = lax.broadcasted_iota(jnp.int32, (8, 2 * LANES), 1) % LANES
        picks = jnp.where(pick(row, column), 1.0, 0.0).astype(jnp.bfloat16)
        return nt(picks, jnp.concatenate([high, low], axis=1))

    def w_arrives(group):
        part = wbuf.at[pl.ds(pl.multiple_of((1 - y) * w_rows, w_rows), w_rows),
                       pl.ds(0, col_part * (1 if group else PAIR))]
        remote(part, part, wy_ssem, wy_rsem.at[group], sp=sp, dp=y_peer).wait_recv()

    def pair_gradients(turn, early):
        pair = pair_of(turn)
        cols = pair_cols(pair)
        with ns(f"pair{turn}a0"):
            if turn:
                w_arrives(0)
                cot_acc[...] = cot_piece(pair, 0, PAIR)
                w_arrives(1)
                cot_acc[...] += cot_piece(pair, PAIR, 1)
                with ns("wy_wait"):
                    w_arrives(2)
            total = cot_acc[...] + cot_piece(pair, n_sp - 1, 1)
            cot = total.astype(jnp.bfloat16)
            cots = [jnp.where(head_mask(sub), cot, 0) for sub in range(per_pair)]
        with ns(f"pair{turn}a1"):
            value_total = [None] * n_blocks
            for sub in range(per_pair):
                h = pair * per_pair + sub
                for b in range(n_blocks):
                    lo, end = b * block, (b + 1) * block
                    add_rows(value_total, nn(prob_b[h, :end, lo:end], cots[sub][lo:end]))
            stage[2, :, cols] = jnp.concatenate(value_total, axis=0).astype(jnp.bfloat16)
            send_grad(2, turn)
        early()
        with ns(f"pair{turn}a2"):
            own_out = o_ref[:, grad_cols(pair)]
            values = v_ref[:, cols]
            dots = picked(cot.astype(jnp.float32) * own_out.astype(jnp.float32),
                          lambda row, column: column // head_width == row)
        key_totals, query_total, row_sums = [], [], []
        for sub in range(per_pair):
            with ns(f"pair{turn}b{sub}"):
                h = pair * per_pair + sub
                spare = jnp.where(lane == (1 - sub) * head_width, 1.0, 0.0).astype(jnp.bfloat16)
                query_h = jnp.where(head_mask(sub), q_ref[:, cols], spare)
                keys_t = k_t[pl.ds(pl.multiple_of(h * head_width, head_width), head_width), :]
                keys_t = jnp.concatenate([keys_t, jnp.ones((16, length), jnp.bfloat16)], axis=0)
                key_total, query_parts = [None] * n_blocks, []
                for b in range(n_blocks):
                    lo, end = b * block, (b + 1) * block
                    weights = prob[h, :end, lo:end]
                    d_prob = nt(values[:end], cots[sub][lo:end])
                    score_b = (weights * (d_prob - dots[sub:sub + 1, lo:end])).astype(jnp.bfloat16)
                    add_rows(key_total, nn(score_b, query_h[lo:end]))
                    query_parts.append(nn(keys_t[:, :end], score_b))
                key_totals.append(jnp.concatenate(key_total, axis=0))
                query_sums = jnp.concatenate(query_parts, axis=1)
                query_total.append(query_sums[:head_width])
                row_sums.append(query_sums[head_width:head_width + 1])
        with ns(f"pair{turn}c"):
            first = head_mask(0)
            key_grad = jnp.where(first, key_totals[0], key_totals[1])
            stage[1, :, cols] = (key_grad * scale).astype(jnp.bfloat16)
            send_grad(1, turn)
            stage[0, :, cols] = (jnp.concatenate(query_total, axis=0).T * scale).astype(jnp.bfloat16)
            send_grad(0, turn)
            col_sums = picked(jnp.where(first, key_totals[1], key_totals[0]),
                              lambda row, column: column == (1 - row) * head_width)
            for sub in range(per_pair):
                d_cum = row_sums[sub] - col_sums[sub:sub + 1]
                dcum_ref[pl.ds(pair * per_pair + sub, 1), :] = d_cum

    def at_step(step):
        return lambda action: pl.when(step_of == step)(action)

    with ns("a_prep"):
        output_transpose()
        key_transpose()
        core_copy(sp).start()
        for h in range(n_heads):
            probabilities(h)

    def relay(first, last):
        for c in range(first, last):
            w_step(c)

    def columns_first(ahead):
        lax.fori_loop(0, ahead, lambda c, done: (w_step(c), done)[1], 0)
        forward_step(0)

        core_copy(core_peer).wait_recv()

    def w_later(c, ahead):
        @pl.when(c >= ahead)
        def _():
            w_step(c)

    def relay2(first, last):
        for c in range(first, last):
            w_later(c, ahead2)

    def relay3(first, last):
        for c in range(first, last):
            w_later(c, ahead3)

    def far_block(n):
        return (2, 5 - n) if n >= 4 else (n % 2, 1 - n // 2)

    def far_near(n):
        step, other = far_block(n)
        value = product(step, other)

        @at_step(3)
        def _():
            to_z(n, value, (0, 1, 2, 3, 7, 4)[n], 2)

        @at_step(2)
        def _():
            dw_part[2 * step + other] = value

    def pass_on(n):
        step, other = n % 2, 1 - n // 2
        to_z(n, part_of(step, other) + from_z(n), 1 - other, step)

    def far_cross(slot, step):
        y_send[slot] = product(step, 1).astype(jnp.bfloat16)

    ahead2 = jnp.where(x == 0, core * w_chunks, 3 - core)
    ahead3 = jnp.where(x == 0, core * w_chunks, 0)

    with ns("b_relay"):
        @pl.when(near)
        def _():
            relay(0, 4)

            @pl.when(core == 0)
            def _():
                forward_step(0)

            for c in range(4, w_chunks):
                w_step(c, c < held)

            @pl.when(core == 1)
            def _():
                forward_step(0)

            core_copy(core_peer).wait_recv()

        @at_step(2)
        def _():
            columns_first(ahead2)

        @at_step(3)
        def _():
            columns_first(ahead3)

    with ns("d_dw"):
        @pl.when(near)
        def _():
            sibling = 1 - step_of
            to_y(0, product(3, 1))
            to_y(1, product(2, 1))
            for c in range(held, w_chunks):
                w_cross(c)
            to_z(0, product(sibling, 1), 2, sibling)
            to_z(1, product(sibling, 0), 3, sibling)
            keep(3, 0)
            keep(2, 0)
            keep(step_of, 1)
            keep(step_of, 0)
            cot_first()
            forward_step(1)
            forward_step(2)
            cot_second()

        @at_step(2)
        def _():
            relay2(0, 1)
            far_near(0)
            relay2(1, 2)
            far_near(1)
            relay2(2, 3)
            far_near(2)
            relay2(3, 4)
            far_near(3)
            relay2(4, 5)
            far_cross(0, 3)
            relay2(5, 6)
            keep(2, 1)
            relay2(6, 7)
            keep(3, 0)
            relay2(7, 8)
            forward_step(1)
            y_copy(0).start()
            keep(2, 0)
            cot_first()
            forward_step(2)
            pass_on(0)
            cot_second()

        @at_step(3)
        def _():
            for n in range(6):
                far_near(n)
            relay3(0, 2)
            far_cross(1, 3)

            @pl.when(x == 0)
            def _():
                forward_step(1)

            relay3(2, 4)
            keep(3, 0)

            @pl.when(x == 1)
            def _():
                forward_step(1)

            @pl.when(x <= core)
            def _():
                forward_step(2)

            relay3(4, 6)

            @pl.when(x > core)
            def _():
                forward_step(2)

            cot_first()
            relay3(6, 7)
            cot_second()
            relay3(7, 8)
            y_copy(1).start()

    with ns("e_cols2"):
        columns_arrive(2)

    def near_far(slot, step):
        return part_of(step, 0) + from_y(slot)

    def over_y():
        to_y(2, part_of(step_of, 1) + from_z(0) + from_z(2))

    with ns("f_poll"):
        @at_step(0)
        def _():
            to_z(2, near_far(0, 3), 4, 1)

        @at_step(1)
        def _():
            dw_part[6] = near_far(0, 3)

        @at_step(2)
        def _():
            pass_on(1)

    def early0():
        with ns("g_poll"):
            @at_step(0)
            def _():
                to_z(3, near_far(1, 2), 5, 2)

            @at_step(1)
            def _():
                to_z(3, near_far(1, 2), 6, 2)

    pair_gradients(0, early0)
    with ns("h_poll"):
        @at_step(2)
        def _():
            pass_on(2)
            pass_on(3)

    def early1():
        with ns("i_poll"):
            @at_step(0)
            def _():
                over_y()

            @at_step(1)
            def _():
                to_z(2, part_of(3, 0) + from_z(4), 5, 3)

            @at_step(2)
            def _():
                to_z(4, part_of(3, 0) + from_y(0), 4, 3)

    pair_gradients(1, early1)
    with ns("j_poll"):
        @at_step(1)
        def _():
            over_y()

        @at_step(2)
        def _():
            to_y(1, part_of(2, 1) + from_z(7))

    with ns("k_final"):
        @pl.when(near)
        def _():
            dw_acc[...] = part_of(step_of, 0) + from_z(1) + from_z(3) + from_y(2)

        @at_step(2)
        def _():
            dw_acc[...] = part_of(2, 0) + from_y(1) + from_z(5) + from_z(6) + from_z(4)

        @at_step(3)
        def _():
            dw_acc[...] = part_of(3, 0) + from_y(1) + from_z(4) + from_z(5)

    results = [
        pltpu.make_async_copy(dw_acc, dw_out, out_sem.at[0]),
        pltpu.make_async_copy(dcum_ref, dcum_out.at[0], out_sem.at[1]),
    ]
    for result in results:
        result.start()

    def sent(part, sem):
        remote(part, part, sem, sem, sp=core_peer, dp=dp).wait_send()

    own_rows = dof.at[token_rows(sp)]
    block_w = wbuf.at[own_w]
    rest = stage.at[:, pl.ds(0, length - tokens)]
    with ns("o_waitsend"):
        sent(own_rows, x_ssem)
        sent(own_rows, f_ssem)
        core_copy(sp).wait_send()
        sent(block_w, wy_ssem)

        @pl.when(sends_up)
        def _():
            sent(block_w, wz_ssem.at[0])

        @pl.when(sends_down)
        def _():
            sent(block_w, wz_ssem.at[1])

        @pl.when(near)
        def _():
            sent(y_send, ry_ssem)
            sent(z_send.at[pl.ds(0, 4)], rz_ssem)

        @at_step(2)
        def _():
            sent(y_send.at[pl.ds(0, 2)], ry_ssem)
            sent(z_send.at[pl.ds(0, 5)], rz_ssem)

        @at_step(3)
        def _():
            sent(y_send.at[pl.ds(0, 1)], ry_ssem)
            sent(z_send, rz_ssem)

        sent(rest, g_ssem)
    with ns("p_gradwait"):
        remote(rest, rest, g_ssem, g_rsem, sp=core_peer, dp=dp).wait_recv()
        kept = stage.at[:, pl.ds(0, tokens)]
        pltpu.make_async_copy(kept, kept, g_lsem).wait()
    with ns("q_results"):
        for result in results:
            result.wait()


def hand_over(*refs):
    count = len(refs) // 2
    copies = [
        pltpu.make_async_copy(refs[i], refs[count + i], refs[-1].at[i]) for i in range(count)
    ]
    for copy in copies:
        copy.start()
    for copy in copies:
        copy.wait()


def fits(mesh, query, cum, d_out, w_out):
    n_sp, n_dp = mesh.shape["sp"], mesh.shape["dp"]
    head_cols, n_heads = query.shape[2] // n_sp, cum.shape[1] // n_sp
    length, width = d_out.shape[1], d_out.shape[2]
    w_rows = w_out.shape[0] // n_dp
    if head_cols % LANES or n_heads == 0 or 8 % n_heads:
        return False
    if LANES != PAIR * (head_cols // n_heads) or length % (2 * LANES) or (width // n_sp) % LANES:
        return False
    if n_sp & (n_sp - 1) or n_sp < PAIR or n_dp != PAIR * n_sp or n_sp != PAIR * PAIR or head_cols != PAIR * LANES or w_rows != LANES:
        return False
    held = 6 * n_heads * length**2 + 2 * length * width + 8 * length * query.shape[2]
    return held < 32 * 2**20


def fused_shards(n_sp, n_dp, query, keys, values, output, cum, d_out, w_out):
    arrays = (query, keys, values, output, cum, d_out, w_out)
    length, head_cols = query.shape[1:]
    attn = output.shape[2]
    n_heads = cum.shape[1]
    tokens, width = d_out.shape[1:]
    w_rows = w_out.shape[0]
    n_z, col_part = n_dp // PAIR, width // n_sp
    w_chunks = 8
    bf16, f32 = jnp.bfloat16, jnp.float32
    dma = pltpu.SemaphoreType.DMA
    n_pairs = head_cols // LANES
    anywhere = pl.BlockSpec(memory_space=pl.ANY)
    from_hbm = pl.BlockSpec(memory_space=pltpu.HBM)
    grad = jax.ShapeDtypeStruct((1, tokens, attn), bf16)
    found = pl.pallas_call(
        functools.partial(kernel, n_sp, n_dp, n_heads, w_chunks),
        out_shape=(
            grad, grad, grad,
            jax.ShapeDtypeStruct(cum.shape, f32),
            jax.ShapeDtypeStruct((w_rows, col_part), f32),
        ),
        in_specs=[from_hbm] * 7,
        out_specs=[anywhere] * 5,
        scratch_shapes=[
            pltpu.VMEM((length, head_cols), bf16),
            pltpu.VMEM((length, head_cols), bf16),
            pltpu.VMEM((length, head_cols), bf16),
            pltpu.VMEM((length, attn), bf16),
            pltpu.VMEM(cum.shape[1:], f32),
            pltpu.VMEM((length, width), bf16),
            pltpu.VMEM((PAIR * w_rows, width), bf16),
            pltpu.VMEM((n_heads, length, length), f32),
            pltpu.VMEM((n_heads, length, length), bf16),
            pltpu.VMEM((head_cols, length), bf16),
            pltpu.VMEM((attn, length), bf16),
            pltpu.VMEM((PAIR * n_z, w_rows, col_part), f32),
            pltpu.VMEM((3, w_rows, col_part), bf16),
            pltpu.VMEM((3, w_rows, col_part), bf16),
            pltpu.VMEM((6, w_rows, col_part), bf16),
            pltpu.VMEM((8, w_rows, col_part), bf16),
            pltpu.VMEM((w_rows, col_part), f32),
            pltpu.VMEM((length, LANES), f32),
            pltpu.VMEM((3, length, head_cols), bf16),
            pltpu.VMEM(cum.shape[1:], f32),
            dma((7,)), dma((2,)),
            dma, dma((n_sp - 1,)), dma, dma, dma, dma((n_sp - 1,)),
            dma((2,)), dma((w_chunks,)), dma, dma((n_sp - 1,)),
            dma, dma((3,)), dma, dma((8,)),
            dma, dma, dma,
        ],
        compiler_params=pltpu.CompilerParams(
            collective_id=0, has_side_effects=True, vmem_limit_bytes=48 * 2**20
        ),
    )(*[pltpu.with_memory_space_constraint(array, pltpu.HBM) for array in arrays])
    return pl.pallas_call(
        hand_over,
        out_shape=[jax.ShapeDtypeStruct(part.shape, part.dtype) for part in found],
        in_specs=[anywhere] * len(found),
        out_specs=[from_hbm] * len(found),
        scratch_shapes=[dma((len(found),))],
        compiler_params=pltpu.CompilerParams(vmem_limit_bytes=2**20),
    )(*found)


def solution(mesh):
    n_sp, n_dp = mesh.shape["sp"], mesh.shape["dp"]
    placed = (
        P("dp", None, "sp"), P("dp", None, "sp"), P("dp", None, "sp"), P("dp", None, None),
        P("dp", "sp", None), P("dp", "sp", None), P("dp", None),
    )
    results = (
        P("dp", "sp", None), P("dp", "sp", None), P("dp", "sp", None), P("dp", "sp", None),
        P("dp", "sp"),
    )

    def run(query, keys, values, output, cum, d_out, w_out):
        if fits(mesh, query, cum, d_out, w_out):
            body = functools.partial(fused_shards, n_sp, n_dp)
            step = jax.shard_map(
                body, mesh=mesh, in_specs=placed, out_specs=results, check_vma=False
            )
        else:
            step = plain_solution(mesh)
        return step(query, keys, values, output, cum, d_out, w_out)

    return run
```

```python
import contextlib
import functools

import jax
import jax.numpy as jnp
from jax import lax
from jax.experimental import pallas as pl
from jax.experimental.pallas import tpu as pltpu
from jax.sharding import PartitionSpec as P


def head_grads(query, keys, values, output, cotangent, cum):
    head_count, length, head_width = query.shape
    span_rows = min(512, length)
    score_scale = head_width ** (-0.5)
    row_dots = jnp.sum(cotangent.astype(jnp.float32) * output.astype(jnp.float32), axis=2)
    positions = jnp.arange(length)

    def product(left, right, form):
        return jnp.einsum(form, left, right, preferred_element_type=jnp.float32)

    def advance(totals, block_index):
        key_grad, value_grad, cum_grad = totals
        offset = block_index * span_rows
        query_blk = lax.dynamic_slice_in_dim(query, offset, span_rows, 1)
        cot_blk = lax.dynamic_slice_in_dim(cotangent, offset, span_rows, 1)
        cum_blk = lax.dynamic_slice_in_dim(cum, offset, span_rows, 1)
        dots_blk = lax.dynamic_slice_in_dim(row_dots, offset, span_rows, 1)
        scores = product(query_blk, keys, "hqe,hke->hqk") * score_scale
        scores = scores + cum_blk[:, :, None] - cum[:, None, :]
        query_pos = offset + jnp.arange(span_rows)
        causal = positions[None, :] <= query_pos[:, None]
        scores = jnp.where(causal[None], scores, -1e30)
        row_max = jnp.max(scores, axis=2, keepdims=True)
        weights = jnp.exp(scores - row_max)
        weights = weights / jnp.sum(weights, axis=2, keepdims=True)
        weights_b = weights.astype(jnp.bfloat16)
        d_prob = product(cot_blk, values, "hqe,hke->hqk")
        d_score = weights * (d_prob - dots_blk[:, :, None])
        score_b = d_score.astype(jnp.bfloat16)
        query_grad = (product(score_b, keys, "hqk,hke->hqe") * score_scale).astype(jnp.bfloat16)
        key_grad = key_grad + product(score_b, query_blk, "hqk,hqe->hke") * score_scale
        value_grad = value_grad + product(weights_b, cot_blk, "hqk,hqe->hke")
        cum_grad = cum_grad - jnp.sum(d_score, axis=1)
        own_part = lax.dynamic_slice_in_dim(cum_grad, offset, span_rows, 1) + jnp.sum(
            d_score, axis=2
        )
        cum_grad = lax.dynamic_update_slice_in_dim(cum_grad, own_part, offset, 1)
        return ((key_grad, value_grad, cum_grad), query_grad)

    start_state = (
        jnp.zeros(query.shape, jnp.float32),
        jnp.zeros(query.shape, jnp.float32),
        jnp.zeros(cum.shape, jnp.float32),
    )
    totals, query_blocks = lax.scan(advance, start_state, jnp.arange(length // span_rows))
    query_grad = jnp.transpose(query_blocks, (1, 0, 2, 3)).reshape(query.shape)
    return (query_grad, totals[0].astype(jnp.bfloat16), totals[1].astype(jnp.bfloat16), totals[2])


def shards(query, keys, values, output, cum, d_out, w_out):
    local_rows = d_out[0]
    whole_output = output[0]
    d_attn = lax.dot_general(
        local_rows,
        lax.all_gather(w_out, "dp", axis=0, tiled=True),
        (((1,), (1,)), ((), ())),
        preferred_element_type=jnp.float32,
    ).astype(jnp.bfloat16)
    head_cot, column_part = (
        lax.all_to_all(d_attn[None], "sp", split_axis=2, concat_axis=1, tiled=True),
        lax.all_to_all(d_out, "sp", split_axis=2, concat_axis=1, tiled=True),
    )
    grad_weight = lax.psum_scatter(
        lax.dot_general(
            whole_output,
            column_part[0],
            (((0,), (0,)), ((), ())),
            preferred_element_type=jnp.float32,
        ),
        "dp",
        scatter_dimension=0,
        tiled=True,
    )
    head_cols = query.shape[2]
    head_count = cum.shape[1]
    head_width = head_cols // head_count
    seq_length = query.shape[1]
    own_output = lax.dynamic_slice_in_dim(
        whole_output, lax.axis_index("sp") * head_cols, head_cols, 1
    )

    def heads_first(matrix):
        return jnp.transpose(matrix.reshape(seq_length, head_count, head_width), (1, 0, 2))

    def tokens_first(matrix):
        return jnp.transpose(matrix, (1, 0, 2)).reshape(1, seq_length, head_cols)

    grads = head_grads(
        heads_first(query[0]),
        heads_first(keys[0]),
        heads_first(values[0]),
        heads_first(own_output),
        heads_first(head_cot[0]),
        cum[0],
    )
    query_grad, key_grad, value_grad = (
        lax.all_to_all(tokens_first(grads[0]), "sp", split_axis=1, concat_axis=2, tiled=True),
        lax.all_to_all(tokens_first(grads[1]), "sp", split_axis=1, concat_axis=2, tiled=True),
        lax.all_to_all(tokens_first(grads[2]), "sp", split_axis=1, concat_axis=2, tiled=True),
    )
    return (query_grad, key_grad, value_grad, grads[3][None], grad_weight)


def plain_solution(mesh):
    placed = (
        P("dp", None, "sp"),
        P("dp", None, "sp"),
        P("dp", None, "sp"),
        P("dp", None, None),
        P("dp", "sp", None),
        P("dp", "sp", None),
        P("dp", None),
    )
    return jax.shard_map(
        shards,
        mesh=mesh,
        in_specs=placed,
        out_specs=(
            P("dp", "sp", None),
            P("dp", "sp", None),
            P("dp", "sp", None),
            P("dp", "sp", None),
            P("dp", "sp"),
        ),
        check_vma=False,
    )


MESH = pl.DeviceIdType.MESH
ns = contextlib.nullcontext
PAIR = 2
LANES = 128


def nt(left, right):
    return lax.dot_general(
        left, right, (((1,), (1,)), ((), ())), preferred_element_type=jnp.float32
    )


def nn(left, right):
    return lax.dot_general(
        left, right, (((1,), (0,)), ((), ())), preferred_element_type=jnp.float32
    )


def kernel(
    n_sp, n_dp, n_heads, w_chunks,
    q_hbm, k_hbm, v_hbm, o_hbm, cum_hbm, do_hbm, w_hbm,
    dq_out, dk_out, dv_out, dcum_out, dw_out,
    q_ref, k_ref, v_ref, o_ref, cum_ref, dof, wbuf, prob, prob_b, k_t, o_t,
    dw_part, y_send, y_recv, z_send, z_recv, dw_acc, cot_acc, stage, dcum_ref,
    in_sem, out_sem,
    x_ssem, x_rsem, c_ssem, c_rsem, f_ssem, f_rsem,
    wz_ssem, wz_rsem, wy_ssem, wy_rsem,
    ry_ssem, ry_rsem, rz_ssem, rz_rsem,
    g_ssem, g_rsem, g_lsem, met_sem,
):
    sp, dp = lax.axis_index("sp"), lax.axis_index("dp")
    n_z = n_dp // PAIR
    x, core = sp // PAIR, sp % PAIR
    z, y = dp // PAIR, dp % PAIR
    length, head_cols = q_ref.shape
    head_width = head_cols // n_heads
    tokens, width = do_hbm.shape[1:]
    w_rows = w_hbm.shape[0]
    col_part = width // n_sp
    scale = head_width ** (-0.5)
    per_pair = LANES // head_width
    n_pairs = head_cols // LANES
    block = min(2 * LANES, length)
    n_blocks = length // block
    core_peer = x * PAIR + (1 - core)
    y_peer = z * PAIR + (1 - y)

    def token_rows(owner):
        return pl.ds(pl.multiple_of(owner * tokens, tokens), tokens)

    def col_at(part):
        return pl.ds(pl.multiple_of(part * col_part, LANES), col_part)

    def remote(src, dst, ssem, rsem, **where):
        return pltpu.make_async_remote_copy(
            src_ref=src, dst_ref=dst, send_sem=ssem, recv_sem=rsem,
            device_id=where, device_id_type=MESH,
        )

    own_w = pl.ds(pl.multiple_of(y * w_rows, w_rows), w_rows)
    loads = [
        pltpu.make_async_copy(do_hbm.at[0], dof.at[token_rows(sp)], in_sem.at[0]),
        pltpu.make_async_copy(q_hbm.at[0], q_ref, in_sem.at[2]),
        pltpu.make_async_copy(k_hbm.at[0], k_ref, in_sem.at[3]),
        pltpu.make_async_copy(cum_hbm.at[0], cum_ref, in_sem.at[4]),
        pltpu.make_async_copy(v_hbm.at[0], v_ref, in_sem.at[5]),
        pltpu.make_async_copy(o_hbm.at[0], o_ref, in_sem.at[6]),
    ]
    w_load = pltpu.make_async_copy(w_hbm, wbuf.at[own_w], in_sem.at[1])
    loads[0].start()

    @pl.when(z == sp)
    def _():
        w_load.start()

    for load in loads[1:]:
        load.start()

    barrier = pltpu.get_barrier_semaphore()
    for off in range(1, n_sp):
        pl.semaphore_signal(
            barrier, inc=1, device_id={"sp": (sp + off) % n_sp, "dp": dp}, device_id_type=MESH
        )
    neighbours = ((z > 0, z - 1), (z < n_z - 1, z + 1))
    n_neighbours = sum(jnp.where(there, 1, 0) for there, _ in neighbours)

    def greet(sem):
        for there, at in neighbours:
            @pl.when(there)
            def _():
                pl.semaphore_signal(
                    sem, inc=1, device_id={"sp": sp, "dp": at * PAIR + y}, device_id_type=MESH
                )

    greet(barrier)
    pl.semaphore_signal(barrier, inc=1, device_id={"sp": sp, "dp": y_peer}, device_id_type=MESH)
    pl.semaphore_wait(barrier, n_sp + n_neighbours)
    greet(met_sem)

    def chip_rows(owner_x):
        return pl.ds(pl.multiple_of(owner_x * PAIR * tokens, PAIR * tokens), PAIR * tokens)

    def x_out(i):
        part = dof.at[token_rows(sp), col_at(((1 - x) * PAIR + i) % n_sp)]
        slot, target_core = (0, i) if i < PAIR else (i - 1, core)
        return remote(part, part, x_ssem, x_rsem.at[slot], sp=(1 - x) * PAIR + target_core, dp=dp)

    def arrived(i, owner_core):
        if i == 0:
            return dof.at[chip_rows(1 - x), col_at(x * PAIR + owner_core)]
        owner = (1 - x) * PAIR + owner_core
        return dof.at[token_rows(owner), col_at((x * PAIR + i + 1) % n_sp)]

    def x_in(i):
        part = arrived(i, core)
        return remote(part, part, x_ssem, x_rsem.at[i], sp=core_peer, dp=dp)

    def core_copy(owner):
        part = dof.at[token_rows(owner)]
        return remote(part, part, c_ssem, c_rsem, sp=core_peer, dp=dp)

    def forward_copy(i, owner_core):
        part = arrived(i, owner_core)
        return remote(part, part, f_ssem, f_rsem.at[i], sp=core_peer, dp=dp)

    def x_start():
        loads[0].wait()
        for i in range(n_sp):
            x_out(i).start()

    def forward_step(i):
        x_in(i).wait_recv()
        forward_copy(i, core).start()

    w_pieces = PAIR * w_chunks
    chunk_cols = width // w_pieces

    def w_part(owner_y, c):
        rows = pl.ds(pl.multiple_of(owner_y * w_rows, w_rows), w_rows)
        start = (x * w_chunks + c) % w_pieces * chunk_cols
        return wbuf.at[rows, pl.ds(pl.multiple_of(start, chunk_cols), chunk_cols)]

    def wz_copy(way, c, target_z):
        return remote(w_part(y, c), w_part(y, c), wz_ssem.at[way], wz_rsem.at[c],
                      sp=sp, dp=target_z * PAIR + y)

    def w_group(c):
        quarter = c * n_sp // w_pieces
        return max(quarter - 1, 0) if isinstance(c, int) else jnp.maximum(quarter - 1, 0)

    def wy_copy(owner_y, c):
        return remote(w_part(owner_y, c), w_part(owner_y, c), wy_ssem, wy_rsem.at[w_group(c)],
                      sp=sp, dp=y_peer)

    sends_up = jnp.logical_and(z >= sp, z < n_z - 1)
    sends_down = jnp.logical_and(z <= sp, z > 0)

    def w_send(c):
        @pl.when(sends_up)
        def _():
            wz_copy(0, c, z + 1).start()

        @pl.when(sends_down)
        def _():
            wz_copy(1, c, z - 1).start()

    def w_cross(c):
        wy_copy(y, c).start()

    near = z // PAIR == x
    far = z // PAIR != x
    held = w_chunks - 3

    @pl.when(z == sp)
    def _():
        w_load.wait()
        for p in range(w_pieces):
            w_send(p)
        x_start()
        for p in range(PAIR * held):
            w_cross(p)

    @pl.when(z != sp)
    def _():
        x_start()

    def pieces_of(c):
        return [PAIR * c + i for i in range(PAIR)]

    def w_step(c, cross=True):
        @pl.when(z != sp)
        def _():
            for p in pieces_of(c):
                wz_copy(0, p, z).wait_recv()
                w_send(p)
                if cross:
                    w_cross(p)

    lane = lax.broadcasted_iota(jnp.int32, (1, LANES), 1)

    def head_mask(sub):
        return lane // head_width == sub

    def pair_cols(pair):
        return pl.ds(pl.multiple_of(pair * LANES, LANES), LANES)

    for load in loads[1:4]:
        load.wait()
    cum = cum_ref[...]
    cum_cols = jnp.concatenate([cum] * (-(-8 // n_heads)), axis=0).T

    def masked_query(pair, sub):
        return jnp.where(head_mask(sub), q_ref[:, pair_cols(pair)], 0)

    def probabilities(h):
        keys = k_ref[:, pair_cols(h // per_pair)]
        query = masked_query(h // per_pair, h % per_pair)
        for b in range(n_blocks):
            lo, end = b * block, (b + 1) * block
            scores = nt(keys[:end], query[lo:end]) * scale
            scores = scores + cum[h:h + 1, lo:end] - cum_cols[:end, h:h + 1]
            key_pos = lax.broadcasted_iota(jnp.int32, (end, block), 0)
            query_pos = lo + lax.broadcasted_iota(jnp.int32, (end, block), 1)
            scores = jnp.where(key_pos <= query_pos, scores, -1e30)
            weights = jnp.exp(scores - jnp.max(scores, axis=0, keepdims=True))
            weights = weights * (1.0 / jnp.sum(weights, axis=0, keepdims=True))
            prob[h, :end, lo:end] = weights
            prob_b[h, :end, lo:end] = weights.astype(jnp.bfloat16)

    def key_transpose():
        k_t[...] = k_ref[...].T

    def output_transpose():
        loads[4].wait()
        loads[5].wait()
        o_t[...] = o_ref[...].T

    step_of = jnp.where(x == 0, z, n_z - 1 - z)

    def dp_at(step, lane_y):
        return jnp.where(x == 0, step, n_z - 1 - step) * PAIR + lane_y

    def lane_of(other):
        return 1 - y if other else y

    def product(step, other):
        row = pl.multiple_of(dp_at(step, lane_of(other)) * w_rows, w_rows)
        return nn(o_t[pl.ds(row, w_rows), :], dof[:, col_at(sp)])

    def keep(step, other):
        dw_part[2 * step + other] = product(step, other)

    def y_copy(slot):
        return remote(y_send.at[slot], y_recv.at[slot], ry_ssem, ry_rsem.at[slot],
                      sp=sp, dp=y_peer)

    def z_copy(source, target, step):
        return remote(z_send.at[source], z_recv.at[target], rz_ssem, rz_rsem.at[target],
                      sp=sp, dp=dp_at(step, y))

    def to_y(slot, value):
        y_send[slot] = value.astype(jnp.bfloat16)
        y_copy(slot).start()

    def to_z(source, value, target, step):
        z_send[source] = value.astype(jnp.bfloat16)
        z_copy(source, target, step).start()

    def from_y(slot):
        y_copy(slot).wait_recv()
        return y_recv[slot].astype(jnp.float32)

    def from_z(target):
        z_copy(0, target, step_of).wait_recv()
        return z_recv[target].astype(jnp.float32)

    def part_of(step, other):
        return dw_part[2 * step + other]

    def pair_of(turn):
        return y if turn == 0 else 1 - y

    def columns_arrive(i):
        forward_copy(i, 1 - core).wait_recv()

    def cot_piece(pair, first, count):
        start = pl.multiple_of((x * PAIR + first) % n_sp * col_part, col_part)
        cols = pl.ds(start, count * col_part)
        return nt(dof[:, cols], wbuf[pl.ds(pl.multiple_of(pair * w_rows, w_rows), w_rows), cols])

    def cot_first():
        columns_arrive(0)
        cot_acc[...] = cot_piece(pair_of(0), 0, PAIR)

    def cot_second():
        columns_arrive(1)
        cot_acc[...] += cot_piece(pair_of(0), PAIR, 1)

    outs = (dq_out, dk_out, dv_out)

    def grad_cols(pair):
        return pl.ds(pl.multiple_of(sp * head_cols + pair * LANES, LANES), LANES)

    def grad_copy(a, turn, target):
        pair = pair_of(turn)
        return remote(stage.at[a, token_rows(target), pair_cols(pair)],
                      outs[a].at[0, :, grad_cols(pair)],
                      g_ssem, g_rsem, sp=target, dp=dp)

    def grad_keep(a, turn):
        pair = pair_of(turn)
        return pltpu.make_async_copy(stage.at[a, token_rows(sp), pair_cols(pair)],
                                     outs[a].at[0, :, grad_cols(pair)], g_lsem)

    def add_rows(totals, part):
        for b in range(part.shape[0] // block):
            piece = part[b * block:(b + 1) * block]
            totals[b] = piece if totals[b] is None else totals[b] + piece

    def send_away(a, turn):
        for i in range(PAIR):
            grad_copy(a, turn, (1 - x) * PAIR + i).start()

    def send_home(a, turn):
        grad_copy(a, turn, core_peer).start()
        grad_keep(a, turn).start()

    def picked(left, pick):
        high = left.astype(jnp.bfloat16)
        low = (left - high.astype(jnp.float32)).astype(jnp.bfloat16)
        row = lax.broadcasted_iota(jnp.int32, (8, 2 * LANES), 0)
        column = lax.broadcasted_iota(jnp.int32, (8, 2 * LANES), 1) % LANES
        picks = jnp.where(pick(row, column), 1.0, 0.0).astype(jnp.bfloat16)
        return nt(picks, jnp.concatenate([high, low], axis=1))

    def w_arrives(group):
        part = wbuf.at[pl.ds(pl.multiple_of((1 - y) * w_rows, w_rows), w_rows),
                       pl.ds(0, col_part * (1 if group else PAIR))]
        remote(part, part, wy_ssem, wy_rsem.at[group], sp=sp, dp=y_peer).wait_recv()

    def score_gradients(turn, cot, cots, side):
        away = 1 - side
        pair = pair_of(turn)
        cols = pair_cols(pair)
        values = v_ref[:, cols]
        with ns(f"pair{turn}a2"):
            own_out = o_ref[:, grad_cols(pair)]
            dots = picked(cot.astype(jnp.float32) * own_out.astype(jnp.float32),
                          lambda row, column: column // head_width == row)
        queries, keys_ts = [], []
        for sub in range(per_pair):
            h = pair * per_pair + sub
            spare = jnp.where(lane == (1 - sub) * head_width, 1.0, 0.0).astype(jnp.bfloat16)
            queries.append(jnp.where(head_mask(sub), q_ref[:, cols], spare))
            keys_t = k_t[pl.ds(pl.multiple_of(h * head_width, head_width), head_width), :]
            keys_ts.append(
                jnp.concatenate([keys_t, jnp.ones((16, length), jnp.bfloat16)], axis=0))
        key_totals = [[None] * n_blocks for _ in range(per_pair)]
        row_sums = [[None] * n_blocks for _ in range(per_pair)]
        first = head_mask(0)

        def finish_keys(b):
            total = jnp.where(first, key_totals[0][b], key_totals[1][b])
            stage[1, b * block:(b + 1) * block, cols] = (total * scale).astype(jnp.bfloat16)
            (send_away if b == away else send_home)(1, turn)

        for b in (away, side):
            with ns(f"pair{turn}b{int(b == side)}"):
                lo, end = b * block, (b + 1) * block
                query_parts = []
                for sub in range(per_pair):
                    weights = prob[pair * per_pair + sub, :end, lo:end]
                    d_prob = nt(values[:end], cots[sub][lo:end])
                    score_b = (weights * (d_prob - dots[sub:sub + 1, lo:end])).astype(jnp.bfloat16)
                    add_rows(key_totals[sub], nn(score_b, queries[sub][lo:end]))
                    query_sums = nn(keys_ts[sub][:, :end], score_b)
                    query_parts.append(query_sums[:head_width])
                    row_sums[sub][b] = query_sums[head_width:head_width + 1]
                if b == n_blocks - 1:
                    finish_keys(away)
                query_grad = jnp.concatenate(query_parts, axis=0).T * scale
                stage[0, lo:end, cols] = query_grad.astype(jnp.bfloat16)
                (send_away if b == away else send_home)(0, turn)
        with ns(f"pair{turn}c"):
            finish_keys(side)
            spare_sums = [jnp.where(first, key_totals[1][b], key_totals[0][b])
                          for b in range(n_blocks)]
            col_sums = picked(jnp.concatenate(spare_sums, axis=0),
                              lambda row, column: column == (1 - row) * head_width)
            for sub in range(per_pair):
                d_cum = jnp.concatenate(row_sums[sub], axis=1) - col_sums[sub:sub + 1]
                dcum_ref[pl.ds(pair * per_pair + sub, 1), :] = d_cum

    def pair_gradients(turn, early):
        pair = pair_of(turn)
        cols = pair_cols(pair)
        with ns(f"pair{turn}a0"):
            if turn:
                w_arrives(0)
                cot_acc[...] = cot_piece(pair, 0, PAIR)
                w_arrives(1)
                cot_acc[...] += cot_piece(pair, PAIR, 1)
                with ns("wy_wait"):
                    w_arrives(2)
            total = cot_acc[...] + cot_piece(pair, n_sp - 1, 1)
            cot = total.astype(jnp.bfloat16)
            cots = [jnp.where(head_mask(sub), cot, 0) for sub in range(per_pair)]
        with ns(f"pair{turn}a1"):
            value_total = [None] * n_blocks
            for sub in range(per_pair):
                h = pair * per_pair + sub
                for b in range(n_blocks):
                    lo, end = b * block, (b + 1) * block
                    add_rows(value_total, nn(prob_b[h, :end, lo:end], cots[sub][lo:end]))
            stage[2, :, cols] = jnp.concatenate(value_total, axis=0).astype(jnp.bfloat16)
            send_away(2, turn)
            send_home(2, turn)
        early()
        for side in range(PAIR):
            @pl.when(x == side)
            def _():
                score_gradients(turn, cot, cots, side)

    def at_step(step):
        return lambda action: pl.when(step_of == step)(action)

    with ns("a_prep"):
        output_transpose()
        key_transpose()
        core_copy(sp).start()
        for h in range(n_heads):
            probabilities(h)

    pl.semaphore_wait(met_sem, n_neighbours)

    def relay(first, last):
        for c in range(first, last):
            w_step(c)

    def columns_first(ahead):
        lax.fori_loop(0, ahead, lambda c, done: (w_step(c), done)[1], 0)
        forward_step(0)

        core_copy(core_peer).wait_recv()

    def w_later(c, ahead):
        @pl.when(c >= ahead)
        def _():
            w_step(c)

    def relay2(first, last):
        for c in range(first, last):
            w_later(c, ahead2)

    def relay3(first, last):
        for c in range(first, last):
            w_later(c, ahead3)

    def far_block(n):
        return (2, 5 - n) if isinstance(n, int) and n >= 4 else (n % 2, 1 - n // 2)

    def far_near(n):
        step, other = far_block(n)
        value = product(step, other)

        @at_step(3)
        def _():
            to_z(n, value, (0, 1, 2, 3, 7, 4)[n], 2)

        @at_step(2)
        def _():
            dw_part[2 * step + other] = value

    def pass_on(n):
        step, other = n % 2, 1 - n // 2
        to_z(n, part_of(step, other) + from_z(n), 1 - other, step)

    def far_cross(slot, step):
        y_send[slot] = product(step, 1).astype(jnp.bfloat16)

    ahead2 = jnp.where(x == 0, core * w_chunks, 3 - core)
    ahead3 = jnp.where(x == 0, core * w_chunks, 0)

    late3 = jnp.logical_and(x == 0, core == 1)

    with ns("b_relay"):
        @pl.when(near)
        def _():
            relay(0, 4)

            @pl.when(core == 0)
            def _():
                forward_step(0)

            for c in range(4, w_chunks):
                w_step(c, c < held)

            @pl.when(core == 1)
            def _():
                forward_step(0)

            core_copy(core_peer).wait_recv()

        @at_step(2)
        def _():
            columns_first(ahead2)

        @at_step(3)
        def _():
            columns_first(jnp.where(late3, 4, ahead3))

    with ns("d_dw"):
        @pl.when(near)
        def _():
            sibling = 1 - step_of
            to_y(0, product(3, 1))
            to_y(1, product(2, 1))
            for p in range(PAIR * held, w_pieces):
                w_cross(p)
            to_z(0, product(sibling, 1), 2, sibling)
            to_z(1, product(sibling, 0), 3, sibling)
            keep(3, 0)
            keep(2, 0)
            keep(step_of, 1)
            keep(step_of, 0)
            cot_first()
            forward_step(1)
            forward_step(2)
            cot_second()

        @at_step(2)
        def _():
            relay2(0, 1)
            far_near(0)
            relay2(1, 2)
            far_near(1)
            relay2(2, 3)
            far_near(2)
            relay2(3, 4)
            far_near(3)
            relay2(4, 5)
            to_y(0, product(3, 1))
            relay2(5, 6)
            keep(2, 1)
            relay2(6, 7)
            keep(3, 0)
            relay2(7, 8)
            forward_step(1)
            keep(2, 0)
            cot_first()
            forward_step(2)

            @pl.when(core == 0)
            def _():
                pass_on(0)

            cot_second()

        @at_step(3)
        def _():
            for n in range(6):
                far_near(n)
                if n < 4:
                    @pl.when(late3)
                    def _():
                        w_step(n + 4)

            relay3(0, 2)
            far_cross(1, 3)

            @pl.when(x == 0)
            def _():
                forward_step(1)

            relay3(2, 4)
            keep(3, 0)

            @pl.when(x == 1)
            def _():
                forward_step(1)

            @pl.when(x <= core)
            def _():
                forward_step(2)

            relay3(4, 6)

            @pl.when(x > core)
            def _():
                forward_step(2)

            cot_first()
            relay3(6, 7)
            cot_second()
            relay3(7, 8)

    with ns("e_cols2"):
        columns_arrive(2)

    def near_far(slot, step):
        return part_of(step, 0) + from_y(slot)

    def far_over_y():
        to_y(1, part_of(2, 1) + from_z(7))

    def over_y():
        to_y(2, part_of(step_of, 1) + from_z(0) + from_z(2))

    with ns("f_poll"):
        @at_step(0)
        def _():
            to_z(2, near_far(0, 3), 4, 1)

        @at_step(1)
        def _():
            dw_part[6] = near_far(0, 3)

        @at_step(2)
        def _():
            pass_on(1 - core)

    def early0():
        with ns("g_poll"):
            @at_step(0)
            def _():
                to_z(3, near_far(1, 2), 5, 2)

            @at_step(1)
            def _():
                to_z(3, near_far(1, 2), 6, 2)

            @at_step(2)
            def _():
                pass_on(2 - core)

    pair_gradients(0, early0)
    with ns("h_poll"):
        @at_step(2)
        def _():
            to_z(4, part_of(3, 0) + from_y(0), 4, 3)
            pass_on(3 - core)

        @at_step(3)
        def _():
            y_copy(1).start()

    def early1():
        with ns("i_poll"):
            @at_step(0)
            def _():
                over_y()

            @at_step(1)
            def _():
                to_z(2, part_of(3, 0) + from_z(4), 5, 3)
                over_y()

            @at_step(2)
            def _():
                @pl.when(core == 0)
                def _():
                    far_over_y()

                @pl.when(core == 1)
                def _():
                    pass_on(3)

    pair_gradients(1, early1)
    with ns("j_poll"):
        @pl.when(jnp.logical_and(step_of == 2, core == 1))
        def _():
            far_over_y()

    with ns("k_final"):
        @pl.when(near)
        def _():
            dw_acc[...] = part_of(step_of, 0) + from_z(1) + from_z(3) + from_y(2)

        @at_step(2)
        def _():
            dw_acc[...] = part_of(2, 0) + from_y(1) + from_z(5) + from_z(6) + from_z(4)

        @at_step(3)
        def _():
            dw_acc[...] = part_of(3, 0) + from_y(1) + from_z(4) + from_z(5)

    results = [
        pltpu.make_async_copy(dw_acc, dw_out, out_sem.at[0]),
        pltpu.make_async_copy(dcum_ref, dcum_out.at[0], out_sem.at[1]),
    ]
    for result in results:
        result.start()

    def sent(part, sem):
        remote(part, part, sem, sem, sp=core_peer, dp=dp).wait_send()

    own_rows = dof.at[token_rows(sp)]
    block_w = wbuf.at[own_w]
    rest = stage.at[:, pl.ds(0, length - tokens)]
    with ns("o_waitsend"):
        sent(own_rows, x_ssem)
        sent(own_rows, f_ssem)
        core_copy(sp).wait_send()
        sent(block_w, wy_ssem)

        @pl.when(sends_up)
        def _():
            sent(block_w, wz_ssem.at[0])

        @pl.when(sends_down)
        def _():
            sent(block_w, wz_ssem.at[1])

        @pl.when(near)
        def _():
            sent(y_send, ry_ssem)
            sent(z_send.at[pl.ds(0, 4)], rz_ssem)

        @at_step(2)
        def _():
            sent(y_send.at[pl.ds(0, 2)], ry_ssem)
            sent(z_send.at[pl.ds(0, 5)], rz_ssem)

        @at_step(3)
        def _():
            sent(y_send.at[pl.ds(0, 1)], ry_ssem)
            sent(z_send, rz_ssem)

        sent(rest, g_ssem)
    with ns("p_gradwait"):
        remote(rest, rest, g_ssem, g_rsem, sp=core_peer, dp=dp).wait_recv()
        kept = stage.at[:, pl.ds(0, tokens)]
        pltpu.make_async_copy(kept, kept, g_lsem).wait()
    with ns("q_results"):
        for result in results:
            result.wait()


def hand_over(*refs):
    count = len(refs) // 2
    copies = [
        pltpu.make_async_copy(refs[i], refs[count + i], refs[-1].at[i]) for i in range(count)
    ]
    for copy in copies:
        copy.start()
    for copy in copies:
        copy.wait()


def fits(mesh, query, cum, d_out, w_out):
    n_sp, n_dp = mesh.shape["sp"], mesh.shape["dp"]
    head_cols, n_heads = query.shape[2] // n_sp, cum.shape[1] // n_sp
    length, width = d_out.shape[1], d_out.shape[2]
    w_rows = w_out.shape[0] // n_dp
    if head_cols % LANES or n_heads == 0 or 8 % n_heads:
        return False
    if LANES != PAIR * (head_cols // n_heads) or length != PAIR * 2 * LANES or (width // n_sp) % LANES:
        return False
    if n_sp & (n_sp - 1) or n_sp < PAIR or n_dp != PAIR * n_sp or n_sp != PAIR * PAIR or head_cols != PAIR * LANES or w_rows != LANES:
        return False
    held = 6 * n_heads * length**2 + 2 * length * width + 8 * length * query.shape[2]
    return held < 32 * 2**20


def fused_shards(n_sp, n_dp, query, keys, values, output, cum, d_out, w_out):
    arrays = (query, keys, values, output, cum, d_out, w_out)
    length, head_cols = query.shape[1:]
    attn = output.shape[2]
    n_heads = cum.shape[1]
    tokens, width = d_out.shape[1:]
    w_rows = w_out.shape[0]
    n_z, col_part = n_dp // PAIR, width // n_sp
    w_chunks = 8
    bf16, f32 = jnp.bfloat16, jnp.float32
    dma = pltpu.SemaphoreType.DMA
    n_pairs = head_cols // LANES
    anywhere = pl.BlockSpec(memory_space=pl.ANY)
    from_hbm = pl.BlockSpec(memory_space=pltpu.HBM)
    grad = jax.ShapeDtypeStruct((1, tokens, attn), bf16)
    found = pl.pallas_call(
        functools.partial(kernel, n_sp, n_dp, n_heads, w_chunks),
        out_shape=(
            grad, grad, grad,
            jax.ShapeDtypeStruct(cum.shape, f32),
            jax.ShapeDtypeStruct((w_rows, col_part), f32),
        ),
        in_specs=[from_hbm] * 7,
        out_specs=[anywhere] * 5,
        scratch_shapes=[
            pltpu.VMEM((length, head_cols), bf16),
            pltpu.VMEM((length, head_cols), bf16),
            pltpu.VMEM((length, head_cols), bf16),
            pltpu.VMEM((length, attn), bf16),
            pltpu.VMEM(cum.shape[1:], f32),
            pltpu.VMEM((length, width), bf16),
            pltpu.VMEM((PAIR * w_rows, width), bf16),
            pltpu.VMEM((n_heads, length, length), f32),
            pltpu.VMEM((n_heads, length, length), bf16),
            pltpu.VMEM((head_cols, length), bf16),
            pltpu.VMEM((attn, length), bf16),
            pltpu.VMEM((PAIR * n_z, w_rows, col_part), f32),
            pltpu.VMEM((3, w_rows, col_part), bf16),
            pltpu.VMEM((3, w_rows, col_part), bf16),
            pltpu.VMEM((6, w_rows, col_part), bf16),
            pltpu.VMEM((8, w_rows, col_part), bf16),
            pltpu.VMEM((w_rows, col_part), f32),
            pltpu.VMEM((length, LANES), f32),
            pltpu.VMEM((3, length, head_cols), bf16),
            pltpu.VMEM(cum.shape[1:], f32),
            dma((7,)), dma((2,)),
            dma, dma((n_sp - 1,)), dma, dma, dma, dma((n_sp - 1,)),
            dma((2,)), dma((PAIR * w_chunks,)), dma, dma((n_sp - 1,)),
            dma, dma((3,)), dma, dma((8,)),
            dma, dma, dma, pltpu.SemaphoreType.REGULAR,
        ],
        compiler_params=pltpu.CompilerParams(
            collective_id=0, has_side_effects=True, vmem_limit_bytes=48 * 2**20
        ),
    )(*[pltpu.with_memory_space_constraint(array, pltpu.HBM) for array in arrays])
    return pl.pallas_call(
        hand_over,
        out_shape=[jax.ShapeDtypeStruct(part.shape, part.dtype) for part in found],
        in_specs=[anywhere] * len(found),
        out_specs=[from_hbm] * len(found),
        scratch_shapes=[dma((len(found),))],
        compiler_params=pltpu.CompilerParams(vmem_limit_bytes=2**20),
    )(*found)


def solution(mesh):
    n_sp, n_dp = mesh.shape["sp"], mesh.shape["dp"]
    placed = (
        P("dp", None, "sp"), P("dp", None, "sp"), P("dp", None, "sp"), P("dp", None, None),
        P("dp", "sp", None), P("dp", "sp", None), P("dp", None),
    )
    results = (
        P("dp", "sp", None), P("dp", "sp", None), P("dp", "sp", None), P("dp", "sp", None),
        P("dp", "sp"),
    )

    def run(query, keys, values, output, cum, d_out, w_out):
        if fits(mesh, query, cum, d_out, w_out):
            body = functools.partial(fused_shards, n_sp, n_dp)
            step = jax.shard_map(
                body, mesh=mesh, in_specs=placed, out_specs=results, check_vma=False
            )
        else:
            step = plain_solution(mesh)
        return step(query, keys, values, output, cum, d_out, w_out)

    return run
```

```python
import contextlib
import functools

import jax
import jax.numpy as jnp
from jax import lax
from jax.experimental import pallas as pl
from jax.experimental.pallas import tpu as pltpu
from jax.sharding import PartitionSpec as P


def head_grads(query, keys, values, output, cotangent, cum):
    head_count, length, head_width = query.shape
    span_rows = min(512, length)
    score_scale = head_width ** (-0.5)
    row_dots = jnp.sum(cotangent.astype(jnp.float32) * output.astype(jnp.float32), axis=2)
    positions = jnp.arange(length)

    def product(left, right, form):
        return jnp.einsum(form, left, right, preferred_element_type=jnp.float32)

    def advance(totals, block_index):
        key_grad, value_grad, cum_grad = totals
        offset = block_index * span_rows
        query_blk = lax.dynamic_slice_in_dim(query, offset, span_rows, 1)
        cot_blk = lax.dynamic_slice_in_dim(cotangent, offset, span_rows, 1)
        cum_blk = lax.dynamic_slice_in_dim(cum, offset, span_rows, 1)
        dots_blk = lax.dynamic_slice_in_dim(row_dots, offset, span_rows, 1)
        scores = product(query_blk, keys, "hqe,hke->hqk") * score_scale
        scores = scores + cum_blk[:, :, None] - cum[:, None, :]
        query_pos = offset + jnp.arange(span_rows)
        causal = positions[None, :] <= query_pos[:, None]
        scores = jnp.where(causal[None], scores, -1e30)
        row_max = jnp.max(scores, axis=2, keepdims=True)
        weights = jnp.exp(scores - row_max)
        weights = weights / jnp.sum(weights, axis=2, keepdims=True)
        weights_b = weights.astype(jnp.bfloat16)
        d_prob = product(cot_blk, values, "hqe,hke->hqk")
        d_score = weights * (d_prob - dots_blk[:, :, None])
        score_b = d_score.astype(jnp.bfloat16)
        query_grad = (product(score_b, keys, "hqk,hke->hqe") * score_scale).astype(jnp.bfloat16)
        key_grad = key_grad + product(score_b, query_blk, "hqk,hqe->hke") * score_scale
        value_grad = value_grad + product(weights_b, cot_blk, "hqk,hqe->hke")
        cum_grad = cum_grad - jnp.sum(d_score, axis=1)
        own_part = lax.dynamic_slice_in_dim(cum_grad, offset, span_rows, 1) + jnp.sum(
            d_score, axis=2
        )
        cum_grad = lax.dynamic_update_slice_in_dim(cum_grad, own_part, offset, 1)
        return ((key_grad, value_grad, cum_grad), query_grad)

    start_state = (
        jnp.zeros(query.shape, jnp.float32),
        jnp.zeros(query.shape, jnp.float32),
        jnp.zeros(cum.shape, jnp.float32),
    )
    totals, query_blocks = lax.scan(advance, start_state, jnp.arange(length // span_rows))
    query_grad = jnp.transpose(query_blocks, (1, 0, 2, 3)).reshape(query.shape)
    return (query_grad, totals[0].astype(jnp.bfloat16), totals[1].astype(jnp.bfloat16), totals[2])


def shards(query, keys, values, output, cum, d_out, w_out):
    local_rows = d_out[0]
    whole_output = output[0]
    d_attn = lax.dot_general(
        local_rows,
        lax.all_gather(w_out, "dp", axis=0, tiled=True),
        (((1,), (1,)), ((), ())),
        preferred_element_type=jnp.float32,
    ).astype(jnp.bfloat16)
    head_cot, column_part = (
        lax.all_to_all(d_attn[None], "sp", split_axis=2, concat_axis=1, tiled=True),
        lax.all_to_all(d_out, "sp", split_axis=2, concat_axis=1, tiled=True),
    )
    grad_weight = lax.psum_scatter(
        lax.dot_general(
            whole_output,
            column_part[0],
            (((0,), (0,)), ((), ())),
            preferred_element_type=jnp.float32,
        ),
        "dp",
        scatter_dimension=0,
        tiled=True,
    )
    head_cols = query.shape[2]
    head_count = cum.shape[1]
    head_width = head_cols // head_count
    seq_length = query.shape[1]
    own_output = lax.dynamic_slice_in_dim(
        whole_output, lax.axis_index("sp") * head_cols, head_cols, 1
    )

    def heads_first(matrix):
        return jnp.transpose(matrix.reshape(seq_length, head_count, head_width), (1, 0, 2))

    def tokens_first(matrix):
        return jnp.transpose(matrix, (1, 0, 2)).reshape(1, seq_length, head_cols)

    grads = head_grads(
        heads_first(query[0]),
        heads_first(keys[0]),
        heads_first(values[0]),
        heads_first(own_output),
        heads_first(head_cot[0]),
        cum[0],
    )
    query_grad, key_grad, value_grad = (
        lax.all_to_all(tokens_first(grads[0]), "sp", split_axis=1, concat_axis=2, tiled=True),
        lax.all_to_all(tokens_first(grads[1]), "sp", split_axis=1, concat_axis=2, tiled=True),
        lax.all_to_all(tokens_first(grads[2]), "sp", split_axis=1, concat_axis=2, tiled=True),
    )
    return (query_grad, key_grad, value_grad, grads[3][None], grad_weight)


def plain_solution(mesh):
    placed = (
        P("dp", None, "sp"),
        P("dp", None, "sp"),
        P("dp", None, "sp"),
        P("dp", None, None),
        P("dp", "sp", None),
        P("dp", "sp", None),
        P("dp", None),
    )
    return jax.shard_map(
        shards,
        mesh=mesh,
        in_specs=placed,
        out_specs=(
            P("dp", "sp", None),
            P("dp", "sp", None),
            P("dp", "sp", None),
            P("dp", "sp", None),
            P("dp", "sp"),
        ),
        check_vma=False,
    )


MESH = pl.DeviceIdType.MESH
ns = contextlib.nullcontext
PAIR = 2
LANES = 128


def nt(left, right):
    return lax.dot_general(
        left, right, (((1,), (1,)), ((), ())), preferred_element_type=jnp.float32
    )


def nn(left, right):
    return lax.dot_general(
        left, right, (((1,), (0,)), ((), ())), preferred_element_type=jnp.float32
    )


def kernel(
    n_sp, n_dp, n_heads, w_chunks,
    q_hbm, k_hbm, v_hbm, o_hbm, cum_hbm, do_hbm, w_hbm,
    dq_out, dk_out, dv_out, dcum_out, dw_out,
    q_ref, k_ref, v_ref, o_ref, cum_ref, dof, wbuf, prob, prob_b, k_t, o_t,
    dw_part, y_send, y_recv, z_send, z_recv, dw_acc, cot_acc, stage, dcum_ref,
    in_sem, out_sem,
    x_ssem, x_rsem, c_ssem, c_rsem, f_ssem, f_rsem,
    wz_ssem, wz_rsem, wy_ssem, wy_rsem,
    ry_ssem, ry_rsem, rz_ssem, rz_rsem,
    g_ssem, g_rsem, g_lsem, met_sem,
    detour, det_ssem, det_rsem,
):
    sp, dp = lax.axis_index("sp"), lax.axis_index("dp")
    n_z = n_dp // PAIR
    x, core = sp // PAIR, sp % PAIR
    z, y = dp // PAIR, dp % PAIR
    length, head_cols = q_ref.shape
    head_width = head_cols // n_heads
    tokens, width = do_hbm.shape[1:]
    w_rows = w_hbm.shape[0]
    col_part = width // n_sp
    scale = head_width ** (-0.5)
    per_pair = LANES // head_width
    n_pairs = head_cols // LANES
    block = min(2 * LANES, length)
    n_blocks = length // block
    core_peer = x * PAIR + (1 - core)
    y_peer = z * PAIR + (1 - y)

    def token_rows(owner):
        return pl.ds(pl.multiple_of(owner * tokens, tokens), tokens)

    def col_at(part):
        return pl.ds(pl.multiple_of(part * col_part, LANES), col_part)

    def remote(src, dst, ssem, rsem, **where):
        return pltpu.make_async_remote_copy(
            src_ref=src, dst_ref=dst, send_sem=ssem, recv_sem=rsem,
            device_id=where, device_id_type=MESH,
        )

    own_w = pl.ds(pl.multiple_of(y * w_rows, w_rows), w_rows)
    loads = [
        pltpu.make_async_copy(do_hbm.at[0], dof.at[token_rows(sp)], in_sem.at[0]),
        pltpu.make_async_copy(q_hbm.at[0], q_ref, in_sem.at[2]),
        pltpu.make_async_copy(k_hbm.at[0], k_ref, in_sem.at[3]),
        pltpu.make_async_copy(cum_hbm.at[0], cum_ref, in_sem.at[4]),
        pltpu.make_async_copy(v_hbm.at[0], v_ref, in_sem.at[5]),
        pltpu.make_async_copy(o_hbm.at[0], o_ref, in_sem.at[6]),
    ]
    w_load = pltpu.make_async_copy(w_hbm, wbuf.at[own_w], in_sem.at[1])
    loads[0].start()

    @pl.when(z == sp)
    def _():
        w_load.start()

    for load in loads[1:]:
        load.start()
    detour_cols = pl.ds(pl.multiple_of((PAIR + n_sp - 1) % n_sp * col_part, col_part), col_part)

    def detour_load():
        return pltpu.make_async_copy(w_hbm.at[:, detour_cols], detour, in_sem.at[7])

    begins = jnp.logical_and(x == 0, z == PAIR + core)
    pl.when(begins)(detour_load().start)

    barrier = pltpu.get_barrier_semaphore()
    for off in range(1, n_sp):
        pl.semaphore_signal(
            barrier, inc=1, device_id={"sp": (sp + off) % n_sp, "dp": dp}, device_id_type=MESH
        )
    neighbours = ((z > 0, z - 1), (z < n_z - 1, z + 1))
    n_neighbours = sum(jnp.where(there, 1, 0) for there, _ in neighbours)

    def greet(sem):
        for there, at in neighbours:
            @pl.when(there)
            def _():
                pl.semaphore_signal(
                    sem, inc=1, device_id={"sp": sp, "dp": at * PAIR + y}, device_id_type=MESH
                )

    greet(barrier)
    pl.semaphore_signal(barrier, inc=1, device_id={"sp": sp, "dp": y_peer}, device_id_type=MESH)
    pl.semaphore_wait(barrier, n_sp + n_neighbours)
    greet(met_sem)

    def chip_rows(owner_x):
        return pl.ds(pl.multiple_of(owner_x * PAIR * tokens, PAIR * tokens), PAIR * tokens)

    def x_out(i):
        part = dof.at[token_rows(sp), col_at(((1 - x) * PAIR + i) % n_sp)]
        slot, target_core = (0, i) if i < PAIR else (i - 1, core)
        return remote(part, part, x_ssem, x_rsem.at[slot], sp=(1 - x) * PAIR + target_core, dp=dp)

    def arrived(i, owner_core):
        if i == 0:
            return dof.at[chip_rows(1 - x), col_at(x * PAIR + owner_core)]
        owner = (1 - x) * PAIR + owner_core
        return dof.at[token_rows(owner), col_at((x * PAIR + i + 1) % n_sp)]

    def x_in(i):
        part = arrived(i, core)
        return remote(part, part, x_ssem, x_rsem.at[i], sp=core_peer, dp=dp)

    def core_copy(owner):
        part = dof.at[token_rows(owner)]
        return remote(part, part, c_ssem, c_rsem, sp=core_peer, dp=dp)

    def forward_copy(i, owner_core):
        part = arrived(i, owner_core)
        return remote(part, part, f_ssem, f_rsem.at[i], sp=core_peer, dp=dp)

    def x_start():
        loads[0].wait()
        for i in range(n_sp):
            x_out(i).start()

    def forward_step(i):
        x_in(i).wait_recv()
        forward_copy(i, core).start()

    w_pieces = PAIR * w_chunks
    chunk_cols = width // w_pieces

    def w_part(owner_y, c):
        rows = pl.ds(pl.multiple_of(owner_y * w_rows, w_rows), w_rows)
        start = (x * w_chunks + c) % w_pieces * chunk_cols
        return wbuf.at[rows, pl.ds(pl.multiple_of(start, chunk_cols), chunk_cols)]

    def wz_copy(way, c, target_z):
        return remote(w_part(y, c), w_part(y, c), wz_ssem.at[way], wz_rsem.at[c],
                      sp=sp, dp=target_z * PAIR + y)

    def w_group(c):
        quarter = c * n_sp // w_pieces
        return max(quarter - 1, 0) if isinstance(c, int) else jnp.maximum(quarter - 1, 0)

    def wy_copy(owner_y, c):
        return remote(w_part(owner_y, c), w_part(owner_y, c), wy_ssem, wy_rsem.at[w_group(c)],
                      sp=sp, dp=y_peer)

    detour_from = w_pieces - w_pieces // n_sp
    skips = jnp.logical_and(x == 1, z == 1)
    detour_rows = pl.ds(pl.multiple_of(y * w_rows, w_rows), w_rows)

    def on(here_z, here_core):
        return jnp.logical_and(x == 0, jnp.logical_and(z == here_z, core == here_core))

    def detour_copy(to_sp, to_z, inside=True):
        target = detour if inside else wbuf.at[detour_rows, detour_cols]
        return remote(detour, target, det_ssem, det_rsem, sp=to_sp, dp=to_z * PAIR + y)

    def detour_first(to_z):
        def run():
            detour_load().wait()
            detour_copy(sp, to_z).start()

        return run

    def detour_relay():
        detour_copy(sp, 0).wait_recv()
        detour_copy(sp, 0).start()

    def detour_cross():
        detour_copy(sp, 0).wait_recv()
        detour_copy(PAIR + core, 0, False).start()

    def detour_take():
        part = wbuf.at[detour_rows, detour_cols]
        remote(part, part, det_ssem, det_rsem, sp=core_peer, dp=dp).wait_recv()
        for p in range(detour_from, w_pieces):
            w_cross(p)

    sends_up = jnp.logical_and(z >= sp, z < n_z - 1)
    sends_down = jnp.logical_and(z <= sp, z > 0)

    def w_send(c):
        @pl.when(sends_up)
        def _():
            wz_copy(0, c, z + 1).start()

        skip = jnp.logical_and(skips, c >= detour_from)

        @pl.when(jnp.logical_and(sends_down, jnp.logical_not(skip)))
        def _():
            wz_copy(1, c, z - 1).start()

    def w_cross(c):
        wy_copy(y, c).start()

    near = z // PAIR == x
    far = z // PAIR != x
    held = w_chunks - 3

    @pl.when(z == sp)
    def _():
        w_load.wait()
        for p in range(w_pieces):
            w_send(p)
        x_start()
        for p in range(PAIR * held):
            w_cross(p)

    @pl.when(z != sp)
    def _():
        x_start()

    def pieces_of(c):
        return [PAIR * c + i for i in range(PAIR)]

    def w_step(c, cross=True):
        @pl.when(z != sp)
        def _():
            for p in pieces_of(c):
                wz_copy(0, p, z).wait_recv()
                w_send(p)
                if cross:
                    w_cross(p)

    lane = lax.broadcasted_iota(jnp.int32, (1, LANES), 1)

    def head_mask(sub):
        return lane // head_width == sub

    def pair_cols(pair):
        return pl.ds(pl.multiple_of(pair * LANES, LANES), LANES)

    for load in loads[1:4]:
        load.wait()
    cum = cum_ref[...]
    cum_cols = jnp.concatenate([cum] * (-(-8 // n_heads)), axis=0).T

    def masked_query(pair, sub):
        return jnp.where(head_mask(sub), q_ref[:, pair_cols(pair)], 0)

    def probabilities(h):
        keys = k_ref[:, pair_cols(h // per_pair)]
        query = masked_query(h // per_pair, h % per_pair)
        for b in range(n_blocks):
            lo, end = b * block, (b + 1) * block
            scores = nt(keys[:end], query[lo:end]) * scale
            scores = scores + cum[h:h + 1, lo:end] - cum_cols[:end, h:h + 1]
            key_pos = lax.broadcasted_iota(jnp.int32, (end, block), 0)
            query_pos = lo + lax.broadcasted_iota(jnp.int32, (end, block), 1)
            scores = jnp.where(key_pos <= query_pos, scores, -1e30)
            weights = jnp.exp(scores - jnp.max(scores, axis=0, keepdims=True))
            weights = weights * (1.0 / jnp.sum(weights, axis=0, keepdims=True))
            prob[h, :end, lo:end] = weights
            prob_b[h, :end, lo:end] = weights.astype(jnp.bfloat16)

    def key_transpose():
        k_t[...] = k_ref[...].T

    def output_transpose():
        loads[4].wait()
        loads[5].wait()
        o_t[...] = o_ref[...].T

    step_of = jnp.where(x == 0, z, n_z - 1 - z)

    def dp_at(step, lane_y):
        return jnp.where(x == 0, step, n_z - 1 - step) * PAIR + lane_y

    def lane_of(other):
        return 1 - y if other else y

    def product(step, other):
        row = pl.multiple_of(dp_at(step, lane_of(other)) * w_rows, w_rows)
        return nn(o_t[pl.ds(row, w_rows), :], dof[:, col_at(sp)])

    def keep(step, other):
        dw_part[2 * step + other] = product(step, other)

    def y_copy(slot):
        return remote(y_send.at[slot], y_recv.at[slot], ry_ssem, ry_rsem.at[slot],
                      sp=sp, dp=y_peer)

    def z_copy(source, target, step):
        return remote(z_send.at[source], z_recv.at[target], rz_ssem, rz_rsem.at[target],
                      sp=sp, dp=dp_at(step, y))

    def to_y(slot, value):
        y_send[slot] = value.astype(jnp.bfloat16)
        y_copy(slot).start()

    def to_z(source, value, target, step):
        z_send[source] = value.astype(jnp.bfloat16)
        z_copy(source, target, step).start()

    def from_y(slot):
        y_copy(slot).wait_recv()
        return y_recv[slot].astype(jnp.float32)

    def from_z(target):
        z_copy(0, target, step_of).wait_recv()
        return z_recv[target].astype(jnp.float32)

    def part_of(step, other):
        return dw_part[2 * step + other]

    def pair_of(turn):
        return y if turn == 0 else 1 - y

    def columns_arrive(i):
        forward_copy(i, 1 - core).wait_recv()

    def cot_piece(pair, first, count):
        start = pl.multiple_of((x * PAIR + first) % n_sp * col_part, col_part)
        cols = pl.ds(start, count * col_part)
        return nt(dof[:, cols], wbuf[pl.ds(pl.multiple_of(pair * w_rows, w_rows), w_rows), cols])

    def cot_first():
        columns_arrive(0)
        cot_acc[...] = cot_piece(pair_of(0), 0, PAIR)

    def cot_second():
        columns_arrive(1)
        cot_acc[...] += cot_piece(pair_of(0), PAIR, 1)

    outs = (dq_out, dk_out, dv_out)

    def grad_cols(pair):
        return pl.ds(pl.multiple_of(sp * head_cols + pair * LANES, LANES), LANES)

    def grad_copy(a, turn, target):
        pair = pair_of(turn)
        return remote(stage.at[a, token_rows(target), pair_cols(pair)],
                      outs[a].at[0, :, grad_cols(pair)],
                      g_ssem, g_rsem, sp=target, dp=dp)

    def grad_keep(a, turn):
        pair = pair_of(turn)
        return pltpu.make_async_copy(stage.at[a, token_rows(sp), pair_cols(pair)],
                                     outs[a].at[0, :, grad_cols(pair)], g_lsem)

    def add_rows(totals, part):
        for b in range(part.shape[0] // block):
            piece = part[b * block:(b + 1) * block]
            totals[b] = piece if totals[b] is None else totals[b] + piece

    def send_away(a, turn):
        for i in range(PAIR):
            grad_copy(a, turn, (1 - x) * PAIR + i).start()

    def send_home(a, turn):
        grad_copy(a, turn, core_peer).start()
        grad_keep(a, turn).start()

    def picked(left, pick):
        high = left.astype(jnp.bfloat16)
        low = (left - high.astype(jnp.float32)).astype(jnp.bfloat16)
        row = lax.broadcasted_iota(jnp.int32, (8, 2 * LANES), 0)
        column = lax.broadcasted_iota(jnp.int32, (8, 2 * LANES), 1) % LANES
        picks = jnp.where(pick(row, column), 1.0, 0.0).astype(jnp.bfloat16)
        return nt(picks, jnp.concatenate([high, low], axis=1))

    def w_arrives(group):
        part = wbuf.at[pl.ds(pl.multiple_of((1 - y) * w_rows, w_rows), w_rows),
                       pl.ds(0, col_part * (1 if group else PAIR))]
        remote(part, part, wy_ssem, wy_rsem.at[group], sp=sp, dp=y_peer).wait_recv()

    def score_gradients(turn, cot, cots, side):
        away = 1 - side
        pair = pair_of(turn)
        cols = pair_cols(pair)
        values = v_ref[:, cols]
        with ns(f"pair{turn}a2"):
            own_out = o_ref[:, grad_cols(pair)]
            dots = picked(cot.astype(jnp.float32) * own_out.astype(jnp.float32),
                          lambda row, column: column // head_width == row)
        queries, keys_ts = [], []
        for sub in range(per_pair):
            h = pair * per_pair + sub
            spare = jnp.where(lane == (1 - sub) * head_width, 1.0, 0.0).astype(jnp.bfloat16)
            queries.append(jnp.where(head_mask(sub), q_ref[:, cols], spare))
            keys_t = k_t[pl.ds(pl.multiple_of(h * head_width, head_width), head_width), :]
            keys_ts.append(
                jnp.concatenate([keys_t, jnp.ones((16, length), jnp.bfloat16)], axis=0))
        key_totals = [[None] * n_blocks for _ in range(per_pair)]
        row_sums = [[None] * n_blocks for _ in range(per_pair)]
        first = head_mask(0)

        def finish_keys(b):
            total = jnp.where(first, key_totals[0][b], key_totals[1][b])
            stage[1, b * block:(b + 1) * block, cols] = (total * scale).astype(jnp.bfloat16)
            (send_away if b == away else send_home)(1, turn)

        for b in (away, side):
            with ns(f"pair{turn}b{int(b == side)}"):
                lo, end = b * block, (b + 1) * block
                query_parts = []
                for sub in range(per_pair):
                    weights = prob[pair * per_pair + sub, :end, lo:end]
                    d_prob = nt(values[:end], cots[sub][lo:end])
                    score_b = (weights * (d_prob - dots[sub:sub + 1, lo:end])).astype(jnp.bfloat16)
                    add_rows(key_totals[sub], nn(score_b, queries[sub][lo:end]))
                    query_sums = nn(keys_ts[sub][:, :end], score_b)
                    query_parts.append(query_sums[:head_width])
                    row_sums[sub][b] = query_sums[head_width:head_width + 1]
                if b == n_blocks - 1:
                    finish_keys(away)
                query_grad = jnp.concatenate(query_parts, axis=0).T * scale
                stage[0, lo:end, cols] = query_grad.astype(jnp.bfloat16)
                (send_away if b == away else send_home)(0, turn)
        with ns(f"pair{turn}c"):
            finish_keys(side)
            spare_sums = [jnp.where(first, key_totals[1][b], key_totals[0][b])
                          for b in range(n_blocks)]
            col_sums = picked(jnp.concatenate(spare_sums, axis=0),
                              lambda row, column: column == (1 - row) * head_width)
            for sub in range(per_pair):
                d_cum = jnp.concatenate(row_sums[sub], axis=1) - col_sums[sub:sub + 1]
                dcum_ref[pl.ds(pair * per_pair + sub, 1), :] = d_cum

    def pair_gradients(turn, early):
        pair = pair_of(turn)
        cols = pair_cols(pair)
        with ns(f"pair{turn}a0"):
            if turn:
                w_arrives(0)
                cot_acc[...] = cot_piece(pair, 0, PAIR)
                w_arrives(1)
                cot_acc[...] += cot_piece(pair, PAIR, 1)
                with ns("wy_wait"):
                    w_arrives(2)
            total = cot_acc[...] + cot_piece(pair, n_sp - 1, 1)
            cot = total.astype(jnp.bfloat16)
            cots = [jnp.where(head_mask(sub), cot, 0) for sub in range(per_pair)]
        with ns(f"pair{turn}a1"):
            value_total = [None] * n_blocks
            for sub in range(per_pair):
                h = pair * per_pair + sub
                for b in range(n_blocks):
                    lo, end = b * block, (b + 1) * block
                    add_rows(value_total, nn(prob_b[h, :end, lo:end], cots[sub][lo:end]))
            stage[2, :, cols] = jnp.concatenate(value_total, axis=0).astype(jnp.bfloat16)
            send_away(2, turn)
            send_home(2, turn)
        early()
        for side in range(PAIR):
            @pl.when(x == side)
            def _():
                score_gradients(turn, cot, cots, side)

    def at_step(step):
        return lambda action: pl.when(step_of == step)(action)

    with ns("a_prep"):
        output_transpose()
        key_transpose()
        core_copy(sp).start()
        for h in range(n_heads):
            probabilities(h)

    pl.semaphore_wait(met_sem, n_neighbours)
    pl.when(on(PAIR, 0))(detour_first(0))
    pl.when(on(PAIR + 1, 1))(detour_first(1))

    def relay(first, last):
        for c in range(first, last):
            w_step(c)

    def columns_first(ahead):
        lax.fori_loop(0, ahead, lambda c, done: (w_step(c), done)[1], 0)
        forward_step(0)

        core_copy(core_peer).wait_recv()

    def w_later(c, ahead):
        @pl.when(c >= ahead)
        def _():
            w_step(c)

    def relay2(first, last):
        for c in range(first, last):
            w_later(c, ahead2)

    def relay3(first, last):
        for c in range(first, last):
            w_later(c, ahead3)

    def far_block(n):
        return (2, 5 - n) if isinstance(n, int) and n >= 4 else (n % 2, 1 - n // 2)

    def far_near(n):
        step, other = far_block(n)
        value = product(step, other)

        @at_step(3)
        def _():
            to_z(n, value, (0, 1, 2, 3, 7, 4)[n], 2)

        @at_step(2)
        def _():
            dw_part[2 * step + other] = value

    def pass_on(n):
        step, other = n % 2, 1 - n // 2
        to_z(n, part_of(step, other) + from_z(n), 1 - other, step)

    def far_cross(slot, step):
        y_send[slot] = product(step, 1).astype(jnp.bfloat16)

    ahead2 = jnp.where(x == 0, core * w_chunks, 3 - 3 * core)
    ahead3 = jnp.where(x == 0, core * w_chunks, 0)

    late3 = jnp.logical_and(x == 0, core == 1)

    with ns("b_relay"):
        @pl.when(near)
        def _():
            def blocks_over_y(between):
                core_copy(core_peer).wait_recv()
                to_y(0, product(3, 1))
                between()
                to_y(1, product(2, 1))

            def cross_held():
                for p in range(PAIR * held, w_pieces):
                    w_cross(p)

            behind = jnp.logical_and(x * core == 1, step_of == 1)
            pl.when(behind)(lambda: w_step(2))
            relay(0, 2)
            pl.when(jnp.logical_not(behind))(lambda: w_step(2))
            relay(3, 4)

            @pl.when(core == 0)
            def _():
                forward_step(0)
                blocks_over_y(lambda: w_step(4))
                relay(5, w_chunks)
                pl.when(z == sp)(cross_held)

            @pl.when(core == 1)
            def _():
                for c in range(4, w_chunks):
                    w_step(c, c < held)
                pl.when(on(1, 1))(detour_relay)
                forward_step(0)
                blocks_over_y(lambda: None)
                cross_held()

        @at_step(2)
        def _():
            columns_first(ahead2)

        @at_step(3)
        def _():
            columns_first(jnp.where(late3, 4, ahead3))

    with ns("d_dw"):
        @pl.when(near)
        def _():
            sibling = 1 - step_of
            to_z(0, product(sibling, 1), 2, sibling)
            to_z(1, product(sibling, 0), 3, sibling)
            keep(3, 0)
            keep(2, 0)
            keep(step_of, 1)
            keep(step_of, 0)
            pl.when(on(0, 0))(detour_cross)
            cot_first()
            forward_step(1)
            forward_step(2)
            cot_second()
            pl.when(on(0, 1))(detour_cross)

        @at_step(2)
        def _():
            relay2(0, 1)
            far_near(0)
            relay2(1, 2)
            far_near(1)
            relay2(2, 3)
            far_near(2)
            relay2(3, 4)
            far_near(3)
            relay2(4, 5)
            to_y(0, product(3, 1))
            relay2(5, 6)

            @pl.when(core == 0)
            def _():
                pass_on(0)
                keep(2, 1)

            @pl.when(core == 1)
            def _():
                far_cross(1, 2)


            @pl.when(x > core)
            def _():
                relay2(6, 8)

            forward_step(1)
            cot_first()

            @pl.when(x <= core)
            def _():
                relay2(6, 7)

            keep(3, 0)
            pl.when(core == 1)(lambda: forward_step(2))

            @pl.when(x <= core)
            def _():
                relay2(7, 8)

            keep(2, 0)

            @pl.when(core == 0)
            def _():
                pass_on(1)
                forward_step(2)


            @pl.when(core == 1)
            def _():
                pass_on(0)

            cot_second()

        @at_step(3)
        def _():
            for n in range(4):
                far_near(n)

                @pl.when(late3)
                def _():
                    w_step(n + 4)

            @pl.when(core == 0)
            def _():
                far_near(4)
                far_near(5)

            @pl.when(core == 1)
            def _():
                far_cross(0, 2)
                keep(2, 0)

            relay3(0, 2)
            far_cross(1, 3)

            @pl.when(x > core)
            def _():
                relay3(2, 5)

            forward_step(1)
            pl.when(x * core == 1)(lambda: forward_step(2))

            @pl.when(x <= core)
            def _():
                relay3(2, 4)

            keep(3, 0)
            pl.when(x == 0)(lambda: forward_step(2))

            @pl.when(x <= core)
            def _():
                relay3(4, 5)

            relay3(5, 6)
            cot_first()
            pl.when(x == 0)(lambda: relay3(6, 7))
            pl.when(x > core)(lambda: forward_step(2))
            pl.when(x > core)(detour_take)
            cot_second()
            pl.when(x * core == 1)(detour_take)
            pl.when(x == 0)(lambda: relay3(7, 8))

            @pl.when(x * core == 1)
            def _():
                y_copy(0).start()

    with ns("e_cols2"):
        columns_arrive(2)

    def near_far(slot, step):
        return part_of(step, 0) + from_y(slot)

    def far_over_y():
        to_y(1, part_of(2, 1) + from_z(7))

    last1 = jnp.logical_and(step_of == 3, core == 1)

    def last_block():
        to_z(5, part_of(2, 0) + from_y(0), 4, 2)

    def over_y():
        to_y(2, part_of(step_of, 1) + from_z(0) + from_z(2))

    with ns("f_poll"):
        @at_step(0)
        def _():
            to_z(2, near_far(0, 3), 4, 1)

        @at_step(1)
        def _():
            dw_part[6] = near_far(0, 3)

    def early0():
        with ns("g_poll"):
            @at_step(0)
            def _():
                to_z(3, near_far(1, 2), 5, 2)

            @at_step(1)
            def _():
                to_z(3, near_far(1, 2), 6, 2)

            @at_step(2)
            def _():
                @pl.when(core == 1)
                def _():
                    pass_on(1)

    pair_gradients(0, early0)
    with ns("h_poll"):
        @at_step(2)
        def _():
            pl.when(core == 1)(y_copy(1).start)
            to_z(4, part_of(3, 0) + from_y(0), 4, 3)
            pass_on(2)

        @at_step(3)
        def _():
            @pl.when(x < core)
            def _():
                y_copy(0).start()

            @pl.when(x == core)
            def _():
                y_copy(1).start()

    def early1():
        with ns("i_poll"):
            @at_step(0)
            def _():
                over_y()

            @at_step(1)
            def _():
                to_z(2, part_of(3, 0) + from_z(4), 5, 3)
                over_y()

            @at_step(2)
            def _():
                pass_on(3)
                pl.when(core == 0)(far_over_y)

            @pl.when(last1)
            def _():
                pl.when(x == 0)(y_copy(1).start)

            @pl.when(jnp.logical_and(step_of == 3, x > core))
            def _():
                y_copy(1).start()

    pair_gradients(1, early1)
    with ns("j_poll"):
        @pl.when(last1)
        def _():
            last_block()

    with ns("k_final"):
        @pl.when(near)
        def _():
            dw_acc[...] = part_of(step_of, 0) + from_z(1) + from_z(3) + from_y(2)

        @at_step(2)
        def _():
            dw_acc[...] = part_of(2, 0) + from_y(1) + from_z(5) + from_z(6) + from_z(4)

        @at_step(3)
        def _():
            dw_acc[...] = part_of(3, 0) + from_y(1) + from_z(4) + from_z(5)

    results = [
        pltpu.make_async_copy(dw_acc, dw_out, out_sem.at[0]),
        pltpu.make_async_copy(dcum_ref, dcum_out.at[0], out_sem.at[1]),
    ]
    for result in results:
        result.start()

    def sent(part, sem):
        remote(part, part, sem, sem, sp=core_peer, dp=dp).wait_send()

    own_rows = dof.at[token_rows(sp)]
    block_w = wbuf.at[own_w]
    rest = stage.at[:, pl.ds(0, length - tokens)]
    with ns("o_waitsend"):
        sent(own_rows, x_ssem)
        sent(own_rows, f_ssem)
        core_copy(sp).wait_send()
        sent(block_w, wy_ssem)

        @pl.when(sends_up)
        def _():
            sent(block_w, wz_ssem.at[0])

        @pl.when(jnp.logical_and(sends_down, jnp.logical_not(skips)))
        def _():
            sent(block_w, wz_ssem.at[1])

        @pl.when(jnp.logical_and(sends_down, skips))
        def _():
            sent(wbuf.at[own_w, pl.ds(0, detour_from * chunk_cols)], wz_ssem.at[1])

        detours = (begins, on(1, 1), jnp.logical_and(x == 0, z == 0))

        @pl.when(functools.reduce(jnp.logical_or, detours))
        def _():
            sent(detour, det_ssem)

        @pl.when(near)
        def _():
            sent(y_send, ry_ssem)
            sent(z_send.at[pl.ds(0, 4)], rz_ssem)

        @at_step(2)
        def _():
            sent(y_send.at[pl.ds(0, 2)], ry_ssem)
            sent(z_send.at[pl.ds(0, 5)], rz_ssem)

        @at_step(3)
        def _():
            @pl.when(core == 0)
            def _():
                sent(y_send.at[pl.ds(0, 1)], ry_ssem)
                sent(z_send, rz_ssem)

            @pl.when(core == 1)
            def _():
                sent(y_send.at[pl.ds(0, 2)], ry_ssem)
                sent(z_send.at[pl.ds(0, 5)], rz_ssem)

        sent(rest, g_ssem)
    with ns("p_gradwait"):
        remote(rest, rest, g_ssem, g_rsem, sp=core_peer, dp=dp).wait_recv()
        kept = stage.at[:, pl.ds(0, tokens)]
        pltpu.make_async_copy(kept, kept, g_lsem).wait()
    with ns("q_results"):
        for result in results:
            result.wait()


def hand_over(*refs):
    count = len(refs) // 2
    copies = [
        pltpu.make_async_copy(refs[i], refs[count + i], refs[-1].at[i]) for i in range(count)
    ]
    for copy in copies:
        copy.start()
    for copy in copies:
        copy.wait()


def fits(mesh, query, cum, d_out, w_out):
    n_sp, n_dp = mesh.shape["sp"], mesh.shape["dp"]
    head_cols, n_heads = query.shape[2] // n_sp, cum.shape[1] // n_sp
    length, width = d_out.shape[1], d_out.shape[2]
    w_rows = w_out.shape[0] // n_dp
    if head_cols % LANES or n_heads == 0 or 8 % n_heads:
        return False
    if LANES != PAIR * (head_cols // n_heads) or length != PAIR * 2 * LANES or (width // n_sp) % LANES:
        return False
    if n_sp & (n_sp - 1) or n_sp < PAIR or n_dp != PAIR * n_sp or n_sp != PAIR * PAIR or head_cols != PAIR * LANES or w_rows != LANES:
        return False
    held = 6 * n_heads * length**2 + 2 * length * width + 8 * length * query.shape[2]
    return held < 32 * 2**20


def fused_shards(n_sp, n_dp, query, keys, values, output, cum, d_out, w_out):
    arrays = (query, keys, values, output, cum, d_out, w_out)
    length, head_cols = query.shape[1:]
    attn = output.shape[2]
    n_heads = cum.shape[1]
    tokens, width = d_out.shape[1:]
    w_rows = w_out.shape[0]
    n_z, col_part = n_dp // PAIR, width // n_sp
    w_chunks = 8
    bf16, f32 = jnp.bfloat16, jnp.float32
    dma = pltpu.SemaphoreType.DMA
    n_pairs = head_cols // LANES
    anywhere = pl.BlockSpec(memory_space=pl.ANY)
    from_hbm = pl.BlockSpec(memory_space=pltpu.HBM)
    grad = jax.ShapeDtypeStruct((1, tokens, attn), bf16)
    found = pl.pallas_call(
        functools.partial(kernel, n_sp, n_dp, n_heads, w_chunks),
        out_shape=(
            grad, grad, grad,
            jax.ShapeDtypeStruct(cum.shape, f32),
            jax.ShapeDtypeStruct((w_rows, col_part), f32),
        ),
        in_specs=[from_hbm] * 7,
        out_specs=[anywhere] * 5,
        scratch_shapes=[
            pltpu.VMEM((length, head_cols), bf16),
            pltpu.VMEM((length, head_cols), bf16),
            pltpu.VMEM((length, head_cols), bf16),
            pltpu.VMEM((length, attn), bf16),
            pltpu.VMEM(cum.shape[1:], f32),
            pltpu.VMEM((length, width), bf16),
            pltpu.VMEM((PAIR * w_rows, width), bf16),
            pltpu.VMEM((n_heads, length, length), f32),
            pltpu.VMEM((n_heads, length, length), bf16),
            pltpu.VMEM((head_cols, length), bf16),
            pltpu.VMEM((attn, length), bf16),
            pltpu.VMEM((PAIR * n_z, w_rows, col_part), f32),
            pltpu.VMEM((3, w_rows, col_part), bf16),
            pltpu.VMEM((3, w_rows, col_part), bf16),
            pltpu.VMEM((6, w_rows, col_part), bf16),
            pltpu.VMEM((8, w_rows, col_part), bf16),
            pltpu.VMEM((w_rows, col_part), f32),
            pltpu.VMEM((length, LANES), f32),
            pltpu.VMEM((3, length, head_cols), bf16),
            pltpu.VMEM(cum.shape[1:], f32),
            dma((8,)), dma((2,)),
            dma, dma((n_sp - 1,)), dma, dma, dma, dma((n_sp - 1,)),
            dma((2,)), dma((PAIR * w_chunks,)), dma, dma((n_sp - 1,)),
            dma, dma((3,)), dma, dma((8,)),
            dma, dma, dma, pltpu.SemaphoreType.REGULAR,
            pltpu.VMEM((w_rows, col_part), bf16), dma, dma,
        ],
        compiler_params=pltpu.CompilerParams(
            collective_id=0, has_side_effects=True, vmem_limit_bytes=48 * 2**20
        ),
    )(*[pltpu.with_memory_space_constraint(array, pltpu.HBM) for array in arrays])
    return pl.pallas_call(
        hand_over,
        out_shape=[jax.ShapeDtypeStruct(part.shape, part.dtype) for part in found],
        in_specs=[anywhere] * len(found),
        out_specs=[from_hbm] * len(found),
        scratch_shapes=[dma((len(found),))],
        compiler_params=pltpu.CompilerParams(vmem_limit_bytes=2**20),
    )(*found)


def solution(mesh):
    n_sp, n_dp = mesh.shape["sp"], mesh.shape["dp"]
    placed = (
        P("dp", None, "sp"), P("dp", None, "sp"), P("dp", None, "sp"), P("dp", None, None),
        P("dp", "sp", None), P("dp", "sp", None), P("dp", None),
    )
    results = (
        P("dp", "sp", None), P("dp", "sp", None), P("dp", "sp", None), P("dp", "sp", None),
        P("dp", "sp"),
    )

    def run(query, keys, values, output, cum, d_out, w_out):
        if fits(mesh, query, cum, d_out, w_out):
            body = functools.partial(fused_shards, n_sp, n_dp)
            step = jax.shard_map(
                body, mesh=mesh, in_specs=placed, out_specs=results, check_vma=False
            )
        else:
            step = plain_solution(mesh)
        return step(query, keys, values, output, cum, d_out, w_out)

    return run
```

```python
import contextlib
import functools

import jax
import jax.numpy as jnp
from jax import lax
from jax.experimental import pallas as pl
from jax.experimental.pallas import tpu as pltpu
from jax.sharding import PartitionSpec as P


def head_grads(query, keys, values, output, cotangent, cum):
    head_count, length, head_width = query.shape
    span_rows = min(512, length)
    score_scale = head_width ** (-0.5)
    row_dots = jnp.sum(cotangent.astype(jnp.float32) * output.astype(jnp.float32), axis=2)
    positions = jnp.arange(length)

    def product(left, right, form):
        return jnp.einsum(form, left, right, preferred_element_type=jnp.float32)

    def advance(totals, block_index):
        key_grad, value_grad, cum_grad = totals
        offset = block_index * span_rows
        query_blk = lax.dynamic_slice_in_dim(query, offset, span_rows, 1)
        cot_blk = lax.dynamic_slice_in_dim(cotangent, offset, span_rows, 1)
        cum_blk = lax.dynamic_slice_in_dim(cum, offset, span_rows, 1)
        dots_blk = lax.dynamic_slice_in_dim(row_dots, offset, span_rows, 1)
        scores = product(query_blk, keys, "hqe,hke->hqk") * score_scale
        scores = scores + cum_blk[:, :, None] - cum[:, None, :]
        query_pos = offset + jnp.arange(span_rows)
        causal = positions[None, :] <= query_pos[:, None]
        scores = jnp.where(causal[None], scores, -1e30)
        row_max = jnp.max(scores, axis=2, keepdims=True)
        weights = jnp.exp(scores - row_max)
        weights = weights / jnp.sum(weights, axis=2, keepdims=True)
        weights_b = weights.astype(jnp.bfloat16)
        d_prob = product(cot_blk, values, "hqe,hke->hqk")
        d_score = weights * (d_prob - dots_blk[:, :, None])
        score_b = d_score.astype(jnp.bfloat16)
        query_grad = (product(score_b, keys, "hqk,hke->hqe") * score_scale).astype(jnp.bfloat16)
        key_grad = key_grad + product(score_b, query_blk, "hqk,hqe->hke") * score_scale
        value_grad = value_grad + product(weights_b, cot_blk, "hqk,hqe->hke")
        cum_grad = cum_grad - jnp.sum(d_score, axis=1)
        own_part = lax.dynamic_slice_in_dim(cum_grad, offset, span_rows, 1) + jnp.sum(
            d_score, axis=2
        )
        cum_grad = lax.dynamic_update_slice_in_dim(cum_grad, own_part, offset, 1)
        return ((key_grad, value_grad, cum_grad), query_grad)

    start_state = (
        jnp.zeros(query.shape, jnp.float32),
        jnp.zeros(query.shape, jnp.float32),
        jnp.zeros(cum.shape, jnp.float32),
    )
    totals, query_blocks = lax.scan(advance, start_state, jnp.arange(length // span_rows))
    query_grad = jnp.transpose(query_blocks, (1, 0, 2, 3)).reshape(query.shape)
    return (query_grad, totals[0].astype(jnp.bfloat16), totals[1].astype(jnp.bfloat16), totals[2])


def shards(query, keys, values, output, cum, d_out, w_out):
    local_rows = d_out[0]
    whole_output = output[0]
    d_attn = lax.dot_general(
        local_rows,
        lax.all_gather(w_out, "dp", axis=0, tiled=True),
        (((1,), (1,)), ((), ())),
        preferred_element_type=jnp.float32,
    ).astype(jnp.bfloat16)
    head_cot, column_part = (
        lax.all_to_all(d_attn[None], "sp", split_axis=2, concat_axis=1, tiled=True),
        lax.all_to_all(d_out, "sp", split_axis=2, concat_axis=1, tiled=True),
    )
    grad_weight = lax.psum_scatter(
        lax.dot_general(
            whole_output,
            column_part[0],
            (((0,), (0,)), ((), ())),
            preferred_element_type=jnp.float32,
        ),
        "dp",
        scatter_dimension=0,
        tiled=True,
    )
    head_cols = query.shape[2]
    head_count = cum.shape[1]
    head_width = head_cols // head_count
    seq_length = query.shape[1]
    own_output = lax.dynamic_slice_in_dim(
        whole_output, lax.axis_index("sp") * head_cols, head_cols, 1
    )

    def heads_first(matrix):
        return jnp.transpose(matrix.reshape(seq_length, head_count, head_width), (1, 0, 2))

    def tokens_first(matrix):
        return jnp.transpose(matrix, (1, 0, 2)).reshape(1, seq_length, head_cols)

    grads = head_grads(
        heads_first(query[0]),
        heads_first(keys[0]),
        heads_first(values[0]),
        heads_first(own_output),
        heads_first(head_cot[0]),
        cum[0],
    )
    query_grad, key_grad, value_grad = (
        lax.all_to_all(tokens_first(grads[0]), "sp", split_axis=1, concat_axis=2, tiled=True),
        lax.all_to_all(tokens_first(grads[1]), "sp", split_axis=1, concat_axis=2, tiled=True),
        lax.all_to_all(tokens_first(grads[2]), "sp", split_axis=1, concat_axis=2, tiled=True),
    )
    return (query_grad, key_grad, value_grad, grads[3][None], grad_weight)


def plain_solution(mesh):
    placed = (
        P("dp", None, "sp"),
        P("dp", None, "sp"),
        P("dp", None, "sp"),
        P("dp", None, None),
        P("dp", "sp", None),
        P("dp", "sp", None),
        P("dp", None),
    )
    return jax.shard_map(
        shards,
        mesh=mesh,
        in_specs=placed,
        out_specs=(
            P("dp", "sp", None),
            P("dp", "sp", None),
            P("dp", "sp", None),
            P("dp", "sp", None),
            P("dp", "sp"),
        ),
        check_vma=False,
    )


MESH = pl.DeviceIdType.MESH
ns = contextlib.nullcontext
PAIR = 2
LANES = 128


def nt(left, right):
    return lax.dot_general(
        left, right, (((1,), (1,)), ((), ())), preferred_element_type=jnp.float32
    )


def nn(left, right):
    return lax.dot_general(
        left, right, (((1,), (0,)), ((), ())), preferred_element_type=jnp.float32
    )


def kernel(
    n_sp, n_dp, n_heads, w_chunks,
    q_hbm, k_hbm, v_hbm, o_hbm, cum_hbm, do_hbm, w_hbm,
    dq_out, dk_out, dv_out, dcum_out, dw_out,
    q_ref, k_ref, v_ref, o_ref, cum_ref, dof, wbuf, prob, prob_b, k_t, o_t,
    dw_part, y_send, y_recv, z_send, z_recv, dw_acc, cot_acc, stage, dcum_ref,
    in_sem, out_sem,
    x_ssem, x_rsem, c_ssem, c_rsem, f_ssem, f_rsem,
    wz_ssem, wz_rsem, wy_ssem, wy_rsem,
    ry_ssem, ry_rsem, rz_ssem, rz_rsem,
    g_ssem, g_rsem, g_lsem, met_sem,
    detour, det_ssem, det_rsem,
):
    sp, dp = lax.axis_index("sp"), lax.axis_index("dp")
    n_z = n_dp // PAIR
    x, core = sp // PAIR, sp % PAIR
    z, y = dp // PAIR, dp % PAIR
    length, head_cols = q_ref.shape
    head_width = head_cols // n_heads
    tokens, width = do_hbm.shape[1:]
    w_rows = w_hbm.shape[0]
    col_part = width // n_sp
    scale = head_width ** (-0.5)
    per_pair = LANES // head_width
    n_pairs = head_cols // LANES
    block = min(2 * LANES, length)
    n_blocks = length // block
    core_peer = x * PAIR + (1 - core)
    y_peer = z * PAIR + (1 - y)

    def token_rows(owner):
        return pl.ds(pl.multiple_of(owner * tokens, tokens), tokens)

    def col_at(part):
        return pl.ds(pl.multiple_of(part * col_part, LANES), col_part)

    def remote(src, dst, ssem, rsem, **where):
        return pltpu.make_async_remote_copy(
            src_ref=src, dst_ref=dst, send_sem=ssem, recv_sem=rsem,
            device_id=where, device_id_type=MESH,
        )

    own_w = pl.ds(pl.multiple_of(y * w_rows, w_rows), w_rows)
    loads = [
        pltpu.make_async_copy(do_hbm.at[0], dof.at[token_rows(sp)], in_sem.at[0]),
        pltpu.make_async_copy(q_hbm.at[0], q_ref, in_sem.at[2]),
        pltpu.make_async_copy(k_hbm.at[0], k_ref, in_sem.at[3]),
        pltpu.make_async_copy(cum_hbm.at[0], cum_ref, in_sem.at[4]),
        pltpu.make_async_copy(v_hbm.at[0], v_ref, in_sem.at[5]),
        pltpu.make_async_copy(o_hbm.at[0], o_ref, in_sem.at[6]),
    ]
    w_load = pltpu.make_async_copy(w_hbm, wbuf.at[own_w], in_sem.at[1])
    loads[0].start()

    @pl.when(z == sp)
    def _():
        w_load.start()

    for load in loads[1:]:
        load.start()
    detour_cols = pl.ds(pl.multiple_of((PAIR + n_sp - 1) % n_sp * col_part, col_part), col_part)

    def detour_load():
        return pltpu.make_async_copy(w_hbm.at[:, detour_cols], detour, in_sem.at[7])

    begins = jnp.logical_and(x == 0, z == PAIR + core)
    pl.when(begins)(detour_load().start)

    barrier = pltpu.get_barrier_semaphore()
    for off in range(1, n_sp):
        pl.semaphore_signal(
            barrier, inc=1, device_id={"sp": (sp + off) % n_sp, "dp": dp}, device_id_type=MESH
        )
    neighbours = ((z > 0, z - 1), (z < n_z - 1, z + 1))
    n_neighbours = sum(jnp.where(there, 1, 0) for there, _ in neighbours)

    def greet(sem):
        for there, at in neighbours:
            @pl.when(there)
            def _():
                pl.semaphore_signal(
                    sem, inc=1, device_id={"sp": sp, "dp": at * PAIR + y}, device_id_type=MESH
                )

    greet(barrier)
    pl.semaphore_signal(barrier, inc=1, device_id={"sp": sp, "dp": y_peer}, device_id_type=MESH)
    pl.semaphore_wait(barrier, n_sp + n_neighbours)
    greet(met_sem)

    def chip_rows(owner_x):
        return pl.ds(pl.multiple_of(owner_x * PAIR * tokens, PAIR * tokens), PAIR * tokens)

    def x_out(i):
        part = dof.at[token_rows(sp), col_at(((1 - x) * PAIR + i) % n_sp)]
        slot, target_core = (0, i) if i < PAIR else (i - 1, core)
        return remote(part, part, x_ssem, x_rsem.at[slot], sp=(1 - x) * PAIR + target_core, dp=dp)

    def arrived(i, owner_core):
        if i == 0:
            return dof.at[chip_rows(1 - x), col_at(x * PAIR + owner_core)]
        owner = (1 - x) * PAIR + owner_core
        return dof.at[token_rows(owner), col_at((x * PAIR + i + 1) % n_sp)]

    def x_in(i):
        part = arrived(i, core)
        return remote(part, part, x_ssem, x_rsem.at[i], sp=core_peer, dp=dp)

    def core_copy(owner):
        part = dof.at[token_rows(owner)]
        return remote(part, part, c_ssem, c_rsem, sp=core_peer, dp=dp)

    def forward_copy(i, owner_core):
        part = arrived(i, owner_core)
        return remote(part, part, f_ssem, f_rsem.at[i], sp=core_peer, dp=dp)

    def x_start():
        loads[0].wait()
        for i in range(n_sp):
            x_out(i).start()

    def forward_step(i):
        x_in(i).wait_recv()
        forward_copy(i, core).start()

    w_pieces = PAIR * w_chunks
    chunk_cols = width // w_pieces

    def w_part(owner_y, c):
        rows = pl.ds(pl.multiple_of(owner_y * w_rows, w_rows), w_rows)
        start = (x * w_chunks + c) % w_pieces * chunk_cols
        return wbuf.at[rows, pl.ds(pl.multiple_of(start, chunk_cols), chunk_cols)]

    def wz_copy(way, c, target_z):
        return remote(w_part(y, c), w_part(y, c), wz_ssem.at[way], wz_rsem.at[c],
                      sp=sp, dp=target_z * PAIR + y)

    def w_group(c):
        quarter = c * n_sp // w_pieces
        return max(quarter - 1, 0) if isinstance(c, int) else jnp.maximum(quarter - 1, 0)

    def wy_copy(owner_y, c):
        return remote(w_part(owner_y, c), w_part(owner_y, c), wy_ssem, wy_rsem.at[w_group(c)],
                      sp=sp, dp=y_peer)

    detour_from = w_pieces - w_pieces // n_sp
    skips = jnp.logical_and(x == 1, z == 1)
    detour_rows = pl.ds(pl.multiple_of(y * w_rows, w_rows), w_rows)

    def on(here_z, here_core):
        return jnp.logical_and(x == 0, jnp.logical_and(z == here_z, core == here_core))

    def detour_copy(to_sp, to_z, inside=True):
        target = detour if inside else wbuf.at[detour_rows, detour_cols]
        return remote(detour, target, det_ssem, det_rsem, sp=to_sp, dp=to_z * PAIR + y)

    def detour_first(to_z):
        def run():
            detour_load().wait()
            detour_copy(sp, to_z).start()

        return run

    def detour_relay():
        detour_copy(sp, 0).wait_recv()
        detour_copy(sp, 0).start()

    def detour_cross():
        detour_copy(sp, 0).wait_recv()
        detour_copy(PAIR + core, 0, False).start()

    def detour_take():
        part = wbuf.at[detour_rows, detour_cols]
        remote(part, part, det_ssem, det_rsem, sp=core_peer, dp=dp).wait_recv()
        for p in range(detour_from, w_pieces):
            w_cross(p)

    sends_up = jnp.logical_and(z >= sp, z < n_z - 1)
    sends_down = jnp.logical_and(z <= sp, z > 0)

    def w_send(c):
        @pl.when(sends_up)
        def _():
            wz_copy(0, c, z + 1).start()

        skip = jnp.logical_and(skips, c >= detour_from)

        @pl.when(jnp.logical_and(sends_down, jnp.logical_not(skip)))
        def _():
            wz_copy(1, c, z - 1).start()

    def w_cross(c):
        wy_copy(y, c).start()

    near = z // PAIR == x
    far = z // PAIR != x
    held = w_chunks - 3

    @pl.when(z == sp)
    def _():
        w_load.wait()
        for p in range(w_pieces):
            w_send(p)
        x_start()
        for p in range(PAIR * held):
            w_cross(p)

    @pl.when(z != sp)
    def _():
        x_start()

    def pieces_of(c):
        return [PAIR * c + i for i in range(PAIR)]

    def w_step(c, cross=True):
        @pl.when(z != sp)
        def _():
            for p in pieces_of(c):
                wz_copy(0, p, z).wait_recv()
                w_send(p)
                if cross:
                    w_cross(p)

    lane = lax.broadcasted_iota(jnp.int32, (1, LANES), 1)

    def head_mask(sub):
        return lane // head_width == sub

    def pair_cols(pair):
        return pl.ds(pl.multiple_of(pair * LANES, LANES), LANES)

    for load in loads[1:4]:
        load.wait()
    cum = cum_ref[...]
    cum_cols = jnp.concatenate([cum] * (-(-8 // n_heads)), axis=0).T

    def masked_query(pair, sub):
        return jnp.where(head_mask(sub), q_ref[:, pair_cols(pair)], 0)

    def probabilities(h):
        keys = k_ref[:, pair_cols(h // per_pair)]
        query = masked_query(h // per_pair, h % per_pair)
        for b in range(n_blocks):
            lo, end = b * block, (b + 1) * block
            scores = nt(keys[:end], query[lo:end]) * scale
            scores = scores + cum[h:h + 1, lo:end] - cum_cols[:end, h:h + 1]
            key_pos = lax.broadcasted_iota(jnp.int32, (end, block), 0)
            query_pos = lo + lax.broadcasted_iota(jnp.int32, (end, block), 1)
            scores = jnp.where(key_pos <= query_pos, scores, -1e30)
            weights = jnp.exp(scores - jnp.max(scores, axis=0, keepdims=True))
            weights = weights * (1.0 / jnp.sum(weights, axis=0, keepdims=True))
            prob[h, :end, lo:end] = weights
            prob_b[h, :end, lo:end] = weights.astype(jnp.bfloat16)

    def key_transpose():
        k_t[...] = k_ref[...].T

    def output_transpose():
        loads[4].wait()
        loads[5].wait()
        o_t[...] = o_ref[...].T

    step_of = jnp.where(x == 0, z, n_z - 1 - z)

    def dp_at(step, lane_y):
        return jnp.where(x == 0, step, n_z - 1 - step) * PAIR + lane_y

    def lane_of(other):
        return 1 - y if other else y

    def product(step, other):
        row = pl.multiple_of(dp_at(step, lane_of(other)) * w_rows, w_rows)
        return nn(o_t[pl.ds(row, w_rows), :], dof[:, col_at(sp)])

    def keep(step, other):
        dw_part[2 * step + other] = product(step, other)

    def y_copy(slot):
        return remote(y_send.at[slot], y_recv.at[slot], ry_ssem, ry_rsem.at[slot],
                      sp=sp, dp=y_peer)

    def z_copy(source, target, step):
        return remote(z_send.at[source], z_recv.at[target], rz_ssem, rz_rsem.at[target],
                      sp=sp, dp=dp_at(step, y))

    def to_y(slot, value):
        y_send[slot] = value.astype(jnp.bfloat16)
        y_copy(slot).start()

    def to_z(source, value, target, step):
        z_send[source] = value.astype(jnp.bfloat16)
        z_copy(source, target, step).start()

    def from_y(slot):
        y_copy(slot).wait_recv()
        return y_recv[slot].astype(jnp.float32)

    def from_z(target):
        z_copy(0, target, step_of).wait_recv()
        return z_recv[target].astype(jnp.float32)

    def part_of(step, other):
        return dw_part[2 * step + other]

    def pair_of(turn):
        return y if turn == 0 else 1 - y

    def columns_arrive(i):
        forward_copy(i, 1 - core).wait_recv()

    def cot_piece(pair, first, count):
        start = pl.multiple_of((x * PAIR + first) % n_sp * col_part, col_part)
        cols = pl.ds(start, count * col_part)
        return nt(dof[:, cols], wbuf[pl.ds(pl.multiple_of(pair * w_rows, w_rows), w_rows), cols])

    def cot_first():
        columns_arrive(0)
        cot_acc[...] = cot_piece(pair_of(0), 0, PAIR)

    def cot_second():
        columns_arrive(1)
        cot_acc[...] += cot_piece(pair_of(0), PAIR, 1)

    outs = (dq_out, dk_out, dv_out)

    def grad_cols(pair):
        return pl.ds(pl.multiple_of(sp * head_cols + pair * LANES, LANES), LANES)

    def grad_copy(a, turn, target):
        pair = pair_of(turn)
        return remote(stage.at[a, token_rows(target), pair_cols(pair)],
                      outs[a].at[0, :, grad_cols(pair)],
                      g_ssem, g_rsem, sp=target, dp=dp)

    def grad_keep(a, turn):
        pair = pair_of(turn)
        return pltpu.make_async_copy(stage.at[a, token_rows(sp), pair_cols(pair)],
                                     outs[a].at[0, :, grad_cols(pair)], g_lsem)

    def add_rows(totals, part):
        for b in range(part.shape[0] // block):
            piece = part[b * block:(b + 1) * block]
            totals[b] = piece if totals[b] is None else totals[b] + piece

    def send_away(a, turn):
        for i in range(PAIR):
            grad_copy(a, turn, (1 - x) * PAIR + i).start()

    def send_home(a, turn):
        grad_copy(a, turn, core_peer).start()
        grad_keep(a, turn).start()

    def picked(left, pick):
        high = left.astype(jnp.bfloat16)
        low = (left - high.astype(jnp.float32)).astype(jnp.bfloat16)
        row = lax.broadcasted_iota(jnp.int32, (8, 2 * LANES), 0)
        column = lax.broadcasted_iota(jnp.int32, (8, 2 * LANES), 1) % LANES
        picks = jnp.where(pick(row, column), 1.0, 0.0).astype(jnp.bfloat16)
        return nt(picks, jnp.concatenate([high, low], axis=1))

    def w_arrives(group):
        part = wbuf.at[pl.ds(pl.multiple_of((1 - y) * w_rows, w_rows), w_rows),
                       pl.ds(0, col_part * (1 if group else PAIR))]
        remote(part, part, wy_ssem, wy_rsem.at[group], sp=sp, dp=y_peer).wait_recv()

    def score_gradients(turn, cot, cots, side):
        away = 1 - side
        pair = pair_of(turn)
        cols = pair_cols(pair)
        values = v_ref[:, cols]
        with ns(f"pair{turn}a2"):
            own_out = o_ref[:, grad_cols(pair)]
            dots = picked(cot.astype(jnp.float32) * own_out.astype(jnp.float32),
                          lambda row, column: column // head_width == row)
        queries, keys_ts = [], []
        for sub in range(per_pair):
            h = pair * per_pair + sub
            spare = jnp.where(lane == (1 - sub) * head_width, 1.0, 0.0).astype(jnp.bfloat16)
            queries.append(jnp.where(head_mask(sub), q_ref[:, cols], spare))
            keys_t = k_t[pl.ds(pl.multiple_of(h * head_width, head_width), head_width), :]
            keys_ts.append(
                jnp.concatenate([keys_t, jnp.ones((16, length), jnp.bfloat16)], axis=0))
        key_totals = [[None] * n_blocks for _ in range(per_pair)]
        row_sums = [[None] * n_blocks for _ in range(per_pair)]
        first = head_mask(0)

        def finish_keys(b):
            total = jnp.where(first, key_totals[0][b], key_totals[1][b])
            stage[1, b * block:(b + 1) * block, cols] = (total * scale).astype(jnp.bfloat16)
            (send_away if b == away else send_home)(1, turn)

        for b in (away, side):
            with ns(f"pair{turn}b{int(b == side)}"):
                lo, end = b * block, (b + 1) * block
                query_parts = []
                for sub in range(per_pair):
                    weights = prob[pair * per_pair + sub, :end, lo:end]
                    d_prob = nt(values[:end], cots[sub][lo:end])
                    score_b = (weights * (d_prob - dots[sub:sub + 1, lo:end])).astype(jnp.bfloat16)
                    add_rows(key_totals[sub], nn(score_b, queries[sub][lo:end]))
                    query_sums = nn(keys_ts[sub][:, :end], score_b)
                    query_parts.append(query_sums[:head_width])
                    row_sums[sub][b] = query_sums[head_width:head_width + 1]
                if b == n_blocks - 1:
                    finish_keys(away)
                query_grad = jnp.concatenate(query_parts, axis=0).T * scale
                stage[0, lo:end, cols] = query_grad.astype(jnp.bfloat16)
                (send_away if b == away else send_home)(0, turn)
        with ns(f"pair{turn}c"):
            finish_keys(side)
            spare_sums = [jnp.where(first, key_totals[1][b], key_totals[0][b])
                          for b in range(n_blocks)]
            col_sums = picked(jnp.concatenate(spare_sums, axis=0),
                              lambda row, column: column == (1 - row) * head_width)
            for sub in range(per_pair):
                d_cum = jnp.concatenate(row_sums[sub], axis=1) - col_sums[sub:sub + 1]
                dcum_ref[pl.ds(pair * per_pair + sub, 1), :] = d_cum

    def pair_gradients(turn, early):
        pair = pair_of(turn)
        cols = pair_cols(pair)
        with ns(f"pair{turn}a0"):
            if turn:
                w_arrives(0)
                cot_acc[...] = cot_piece(pair, 0, PAIR)
                w_arrives(1)
                cot_acc[...] += cot_piece(pair, PAIR, 1)
                with ns("wy_wait"):
                    w_arrives(2)
            total = cot_acc[...] + cot_piece(pair, n_sp - 1, 1)
            cot = total.astype(jnp.bfloat16)
            cots = [jnp.where(head_mask(sub), cot, 0) for sub in range(per_pair)]
        def value_gradients():
            with ns(f"pair{turn}a1"):
                value_total = [None] * n_blocks
                for sub in range(per_pair):
                    h = pair * per_pair + sub
                    for b in range(n_blocks):
                        lo, end = b * block, (b + 1) * block
                        add_rows(value_total, nn(prob_b[h, :end, lo:end], cots[sub][lo:end]))
                stage[2, :, cols] = jnp.concatenate(value_total, axis=0).astype(jnp.bfloat16)
                send_away(2, turn)
                send_home(2, turn)

        early()
        for side in range(PAIR):
            @pl.when(x == side)
            def _():
                value_gradients()
                score_gradients(turn, cot, cots, side)

    def at_step(step):
        return lambda action: pl.when(step_of == step)(action)

    with ns("a_prep"):
        output_transpose()
        key_transpose()
        core_copy(sp).start()
        for h in range(n_heads):
            probabilities(h)

    pl.semaphore_wait(met_sem, n_neighbours)
    pl.when(on(PAIR, 0))(detour_first(0))
    pl.when(on(PAIR + 1, 1))(detour_first(1))

    def relay(first, last):
        for c in range(first, last):
            w_step(c)

    def columns_first(ahead):
        lax.fori_loop(0, ahead, lambda c, done: (w_step(c), done)[1], 0)
        forward_step(0)

        core_copy(core_peer).wait_recv()

    def w_later(c, ahead):
        @pl.when(c >= ahead)
        def _():
            w_step(c)

    def relay2(first, last):
        for c in range(first, last):
            w_later(c, ahead2)

    def relay3(first, last):
        for c in range(first, last):
            w_later(c, ahead3)

    def far_block(n):
        return (2, 5 - n) if isinstance(n, int) and n >= 4 else (n % 2, 1 - n // 2)

    def far_near(n):
        step, other = far_block(n)
        value = product(step, other)

        @at_step(3)
        def _():
            to_z(n, value, (0, 1, 2, 3, 7, 4)[n], 2)

        @at_step(2)
        def _():
            dw_part[2 * step + other] = value

    def pass_on(n):
        step, other = n % 2, 1 - n // 2
        to_z(n, part_of(step, other) + from_z(n), 1 - other, step)

    def far_cross(slot, step):
        y_send[slot] = product(step, 1).astype(jnp.bfloat16)

    ahead2 = jnp.where(x == 0, core * w_chunks, 3 - 3 * core)
    ahead3 = jnp.where(x == 0, core * w_chunks, 0)

    late3 = jnp.logical_and(x == 0, core == 1)

    with ns("b_relay"):
        @pl.when(near)
        def _():
            def blocks_over_y(between):
                core_copy(core_peer).wait_recv()
                to_y(0, product(3, 1))
                between()
                to_y(1, product(2, 1))

            def cross_held():
                for p in range(PAIR * held, w_pieces):
                    w_cross(p)

            behind = jnp.logical_and(x * core == 1, step_of == 1)
            pl.when(behind)(lambda: w_step(2))
            relay(0, 2)
            pl.when(jnp.logical_not(behind))(lambda: w_step(2))
            relay(3, 4)

            @pl.when(core == 0)
            def _():
                forward_step(0)
                blocks_over_y(lambda: w_step(4))
                relay(5, w_chunks)
                pl.when(z == sp)(cross_held)

            @pl.when(core == 1)
            def _():
                for c in range(4, w_chunks):
                    w_step(c, c < held)
                pl.when(on(1, 1))(detour_relay)
                forward_step(0)
                blocks_over_y(lambda: None)
                cross_held()

        @at_step(2)
        def _():
            columns_first(ahead2)

        @at_step(3)
        def _():
            columns_first(jnp.where(late3, 4, ahead3))

    with ns("d_dw"):
        @pl.when(near)
        def _():
            sibling = 1 - step_of
            to_z(0, product(sibling, 1), 2, sibling)
            to_z(1, product(sibling, 0), 3, sibling)
            keep(3, 0)
            keep(2, 0)
            keep(step_of, 1)
            keep(step_of, 0)
            pl.when(on(0, 0))(detour_cross)
            cot_first()
            forward_step(1)
            forward_step(2)
            cot_second()
            pl.when(on(0, 1))(detour_cross)

        @at_step(2)
        def _():
            relay2(0, 1)
            far_near(0)
            relay2(1, 2)
            far_near(1)
            relay2(2, 3)
            far_near(2)
            relay2(3, 4)
            far_near(3)
            relay2(4, 5)
            to_y(0, product(3, 1))
            relay2(5, 6)

            @pl.when(core == 0)
            def _():
                pass_on(0)
                keep(2, 1)

            @pl.when(core == 1)
            def _():
                far_cross(1, 2)


            @pl.when(x > core)
            def _():
                relay2(6, 8)

            forward_step(1)
            cot_first()

            @pl.when(x <= core)
            def _():
                relay2(6, 7)

            keep(3, 0)
            pl.when(core == 1)(lambda: forward_step(2))

            @pl.when(x <= core)
            def _():
                relay2(7, 8)

            keep(2, 0)

            @pl.when(core == 0)
            def _():
                pass_on(1)
                forward_step(2)


            @pl.when(core == 1)
            def _():
                pass_on(0)

            cot_second()

        @at_step(3)
        def _():
            for n in range(4):
                far_near(n)

                @pl.when(late3)
                def _():
                    w_step(n + 4)

            @pl.when(core == 0)
            def _():
                far_near(4)
                far_near(5)

            @pl.when(core == 1)
            def _():
                far_cross(0, 2)
                keep(2, 0)

            relay3(0, 2)
            far_cross(1, 3)

            @pl.when(x > core)
            def _():
                relay3(2, 5)

            forward_step(1)
            pl.when(x * core == 1)(lambda: forward_step(2))

            @pl.when(x <= core)
            def _():
                relay3(2, 4)

            keep(3, 0)
            pl.when(x == 0)(lambda: forward_step(2))

            @pl.when(x <= core)
            def _():
                relay3(4, 5)

            relay3(5, 6)
            cot_first()
            pl.when(x == 0)(lambda: relay3(6, 7))
            pl.when(x > core)(lambda: forward_step(2))
            pl.when(x > core)(detour_take)
            cot_second()
            pl.when(x * core == 1)(detour_take)
            pl.when(x == 0)(lambda: relay3(7, 8))

            @pl.when(x * core == 1)
            def _():
                y_copy(0).start()

    with ns("e_cols2"):
        columns_arrive(2)

    def near_far(slot, step):
        return part_of(step, 0) + from_y(slot)

    def far_over_y():
        to_y(1, part_of(2, 1) + from_z(7))

    last1 = jnp.logical_and(step_of == 3, core == 1)

    def last_block():
        to_z(5, part_of(2, 0) + from_y(0), 4, 2)

    def over_y():
        to_y(2, part_of(step_of, 1) + from_z(0) + from_z(2))

    with ns("f_poll"):
        @at_step(0)
        def _():
            to_z(2, near_far(0, 3), 4, 1)

        @at_step(1)
        def _():
            dw_part[6] = near_far(0, 3)

    def early0():
        with ns("g_poll"):
            @at_step(0)
            def _():
                to_z(3, near_far(1, 2), 5, 2)

            @at_step(1)
            def _():
                to_z(3, near_far(1, 2), 6, 2)

            @at_step(2)
            def _():
                @pl.when(core == 1)
                def _():
                    pass_on(1)

    pair_gradients(0, early0)
    with ns("h_poll"):
        @at_step(2)
        def _():
            pl.when(core == 1)(y_copy(1).start)
            to_z(4, part_of(3, 0) + from_y(0), 4, 3)
            pass_on(2)

        @at_step(3)
        def _():
            @pl.when(x < core)
            def _():
                y_copy(0).start()

            @pl.when(x == core)
            def _():
                y_copy(1).start()

    def early1():
        with ns("i_poll"):
            @at_step(0)
            def _():
                over_y()

            @at_step(1)
            def _():
                to_z(2, part_of(3, 0) + from_z(4), 5, 3)
                over_y()

            @at_step(2)
            def _():
                pass_on(3)
                pl.when(core == 0)(far_over_y)

            @pl.when(last1)
            def _():
                pl.when(x == 0)(y_copy(1).start)

            @pl.when(jnp.logical_and(step_of == 3, x > core))
            def _():
                y_copy(1).start()

    pair_gradients(1, early1)
    with ns("j_poll"):
        @pl.when(last1)
        def _():
            last_block()

    with ns("k_final"):
        @pl.when(near)
        def _():
            dw_acc[...] = part_of(step_of, 0) + from_z(1) + from_z(3) + from_y(2)

        @at_step(2)
        def _():
            dw_acc[...] = part_of(2, 0) + from_y(1) + from_z(5) + from_z(6) + from_z(4)

        @at_step(3)
        def _():
            dw_acc[...] = part_of(3, 0) + from_y(1) + from_z(4) + from_z(5)

    results = [
        pltpu.make_async_copy(dw_acc, dw_out, out_sem.at[0]),
        pltpu.make_async_copy(dcum_ref, dcum_out.at[0], out_sem.at[1]),
    ]
    for result in results:
        result.start()

    def sent(part, sem):
        remote(part, part, sem, sem, sp=core_peer, dp=dp).wait_send()

    own_rows = dof.at[token_rows(sp)]
    block_w = wbuf.at[own_w]
    rest = stage.at[:, pl.ds(0, length - tokens)]
    with ns("o_waitsend"):
        sent(own_rows, x_ssem)
        sent(own_rows, f_ssem)
        core_copy(sp).wait_send()
        sent(block_w, wy_ssem)

        @pl.when(sends_up)
        def _():
            sent(block_w, wz_ssem.at[0])

        @pl.when(jnp.logical_and(sends_down, jnp.logical_not(skips)))
        def _():
            sent(block_w, wz_ssem.at[1])

        @pl.when(jnp.logical_and(sends_down, skips))
        def _():
            sent(wbuf.at[own_w, pl.ds(0, detour_from * chunk_cols)], wz_ssem.at[1])

        detours = (begins, on(1, 1), jnp.logical_and(x == 0, z == 0))

        @pl.when(functools.reduce(jnp.logical_or, detours))
        def _():
            sent(detour, det_ssem)

        @pl.when(near)
        def _():
            sent(y_send, ry_ssem)
            sent(z_send.at[pl.ds(0, 4)], rz_ssem)

        @at_step(2)
        def _():
            sent(y_send.at[pl.ds(0, 2)], ry_ssem)
            sent(z_send.at[pl.ds(0, 5)], rz_ssem)

        @at_step(3)
        def _():
            @pl.when(core == 0)
            def _():
                sent(y_send.at[pl.ds(0, 1)], ry_ssem)
                sent(z_send, rz_ssem)

            @pl.when(core == 1)
            def _():
                sent(y_send.at[pl.ds(0, 2)], ry_ssem)
                sent(z_send.at[pl.ds(0, 5)], rz_ssem)

        sent(rest, g_ssem)
    with ns("p_gradwait"):
        remote(rest, rest, g_ssem, g_rsem, sp=core_peer, dp=dp).wait_recv()
        kept = stage.at[:, pl.ds(0, tokens)]
        pltpu.make_async_copy(kept, kept, g_lsem).wait()
    with ns("q_results"):
        for result in results:
            result.wait()


def hand_over(*refs):
    count = len(refs) // 2
    copies = [
        pltpu.make_async_copy(refs[i], refs[count + i], refs[-1].at[i]) for i in range(count)
    ]
    for copy in copies:
        copy.start()
    for copy in copies:
        copy.wait()


def fits(mesh, query, cum, d_out, w_out):
    n_sp, n_dp = mesh.shape["sp"], mesh.shape["dp"]
    head_cols, n_heads = query.shape[2] // n_sp, cum.shape[1] // n_sp
    length, width = d_out.shape[1], d_out.shape[2]
    w_rows = w_out.shape[0] // n_dp
    if head_cols % LANES or n_heads == 0 or 8 % n_heads:
        return False
    if LANES != PAIR * (head_cols // n_heads) or length != PAIR * 2 * LANES or (width // n_sp) % LANES:
        return False
    if n_sp & (n_sp - 1) or n_sp < PAIR or n_dp != PAIR * n_sp or n_sp != PAIR * PAIR or head_cols != PAIR * LANES or w_rows != LANES:
        return False
    held = 6 * n_heads * length**2 + 2 * length * width + 8 * length * query.shape[2]
    return held < 32 * 2**20


def fused_shards(n_sp, n_dp, query, keys, values, output, cum, d_out, w_out):
    arrays = (query, keys, values, output, cum, d_out, w_out)
    length, head_cols = query.shape[1:]
    attn = output.shape[2]
    n_heads = cum.shape[1]
    tokens, width = d_out.shape[1:]
    w_rows = w_out.shape[0]
    n_z, col_part = n_dp // PAIR, width // n_sp
    w_chunks = 8
    bf16, f32 = jnp.bfloat16, jnp.float32
    dma = pltpu.SemaphoreType.DMA
    n_pairs = head_cols // LANES
    anywhere = pl.BlockSpec(memory_space=pl.ANY)
    from_hbm = pl.BlockSpec(memory_space=pltpu.HBM)
    grad = jax.ShapeDtypeStruct((1, tokens, attn), bf16)
    found = pl.pallas_call(
        functools.partial(kernel, n_sp, n_dp, n_heads, w_chunks),
        out_shape=(
            grad, grad, grad,
            jax.ShapeDtypeStruct(cum.shape, f32),
            jax.ShapeDtypeStruct((w_rows, col_part), f32),
        ),
        in_specs=[from_hbm] * 7,
        out_specs=[anywhere] * 5,
        scratch_shapes=[
            pltpu.VMEM((length, head_cols), bf16),
            pltpu.VMEM((length, head_cols), bf16),
            pltpu.VMEM((length, head_cols), bf16),
            pltpu.VMEM((length, attn), bf16),
            pltpu.VMEM(cum.shape[1:], f32),
            pltpu.VMEM((length, width), bf16),
            pltpu.VMEM((PAIR * w_rows, width), bf16),
            pltpu.VMEM((n_heads, length, length), f32),
            pltpu.VMEM((n_heads, length, length), bf16),
            pltpu.VMEM((head_cols, length), bf16),
            pltpu.VMEM((attn, length), bf16),
            pltpu.VMEM((PAIR * n_z, w_rows, col_part), f32),
            pltpu.VMEM((3, w_rows, col_part), bf16),
            pltpu.VMEM((3, w_rows, col_part), bf16),
            pltpu.VMEM((6, w_rows, col_part), bf16),
            pltpu.VMEM((8, w_rows, col_part), bf16),
            pltpu.VMEM((w_rows, col_part), f32),
            pltpu.VMEM((length, LANES), f32),
            pltpu.VMEM((3, length, head_cols), bf16),
            pltpu.VMEM(cum.shape[1:], f32),
            dma((8,)), dma((2,)),
            dma, dma((n_sp - 1,)), dma, dma, dma, dma((n_sp - 1,)),
            dma((2,)), dma((PAIR * w_chunks,)), dma, dma((n_sp - 1,)),
            dma, dma((3,)), dma, dma((8,)),
            dma, dma, dma, pltpu.SemaphoreType.REGULAR,
            pltpu.VMEM((w_rows, col_part), bf16), dma, dma,
        ],
        compiler_params=pltpu.CompilerParams(
            collective_id=0, has_side_effects=True, vmem_limit_bytes=48 * 2**20
        ),
    )(*[pltpu.with_memory_space_constraint(array, pltpu.HBM) for array in arrays])
    return pl.pallas_call(
        hand_over,
        out_shape=[jax.ShapeDtypeStruct(part.shape, part.dtype) for part in found],
        in_specs=[anywhere] * len(found),
        out_specs=[from_hbm] * len(found),
        scratch_shapes=[dma((len(found),))],
        compiler_params=pltpu.CompilerParams(vmem_limit_bytes=2**20),
    )(*found)


def solution(mesh):
    n_sp, n_dp = mesh.shape["sp"], mesh.shape["dp"]
    placed = (
        P("dp", None, "sp"), P("dp", None, "sp"), P("dp", None, "sp"), P("dp", None, None),
        P("dp", "sp", None), P("dp", "sp", None), P("dp", None),
    )
    results = (
        P("dp", "sp", None), P("dp", "sp", None), P("dp", "sp", None), P("dp", "sp", None),
        P("dp", "sp"),
    )

    def run(query, keys, values, output, cum, d_out, w_out):
        if fits(mesh, query, cum, d_out, w_out):
            body = functools.partial(fused_shards, n_sp, n_dp)
            step = jax.shard_map(
                body, mesh=mesh, in_specs=placed, out_specs=results, check_vma=False
            )
        else:
            step = plain_solution(mesh)
        return step(query, keys, values, output, cum, d_out, w_out)

    return run
```
